32 devices in a mesh: ep: 8 (over z, x), tp: 4 (over y, core).
Axes of the slice: x: 2, y: 2, z: 4, core: 2. Of those that a mesh axis runs over, the one named last changes fastest.
Arguments:
- tokens: bfloat16 [1024, 2048], P('ep', 'tp'), may hold values from -6 to 6
- cotangent: bfloat16 [1024, 2048], P('ep', 'tp'), may hold values from -6 to 6
- experts: int32 [1024, 2], P('ep'), may hold values from 0 to 7, as said below
- combine: float32 [1024, 2], P('ep'), may hold values from 0.2 to 1
- w_gate: bfloat16 [8, 2048, 256], P('ep', 'tp'), may hold values from -0.125 to 0.125
- w_up: bfloat16 [8, 2048, 256], P('ep', 'tp'), may hold values from -0.125 to 0.125
- w_down: bfloat16 [8, 256, 2048], P('ep', None, 'tp'), may hold values from -0.375 to 0.375
Outputs:
- grad_tokens: bfloat16 [1024, 2048], P('ep', 'tp')
- grad_combine: float32 [1024, 2], P('ep')
- gate_grad: float32 [8, 2048, 256], P('ep', 'tp')
- up_grad: float32 [8, 2048, 256], P('ep', 'tp')
- down_grad: float32 [8, 256, 2048], P('ep', None, 'tp')
The draws below stay inside these ranges and needn't reach their ends.
Inputs may be any that keep to these rules, and one draw needn't show every extreme that they name: Each row names two different experts of one group of 4 consecutive experts. The rows of one index of ep name any one expert at most 64 times, and some expert exactly 64 times.
All inputs are finite; a program needn't handle non-finite values.
Results may differ from the reference program's by a relative error of at most 0.019.
Values may be sent and summed in bfloat16 or wider, within the bound.
A program may use at most 64 MiB of HBM per device.

```python
import jax
import jax.numpy as jnp
from jax import lax

D = 2048
FE = 256
TOPK = 2
GSIZE = 4
TOK_DEV = 128
TOKENS = 1024
EXPERTS = 8
GROUPS = 2
CAP = 64
N_EP = 8
N_TP = 4


def draw_experts(key, part):
    base_group = jax.random.randint(jax.random.fold_in(key, 7), (), 0, GROUPS).astype(jnp.int32)
    device_keys = jax.random.split(jax.random.fold_in(key, 11), N_EP)
    device_ids = jnp.arange(N_EP, dtype=jnp.int32)

    def one_device(device_key, device_id):
        keys_four = jax.random.split(device_key, 4)
        hot_group = ((base_group + device_id) % GROUPS).astype(jnp.int32)
        pair_count = GROUPS // 2
        step_range = CAP // 4
        shifts = 4 * jax.random.randint(keys_four[0], (pair_count,), -step_range, step_range + 1).astype(jnp.int32)
        shifts = shifts.at[0].set(CAP)
        quotas = jnp.stack([CAP + shifts, CAP - shifts], axis=1).reshape(GROUPS).astype(jnp.int32)
        others = (hot_group + 1 + jnp.arange(GROUPS - 1, dtype=jnp.int32)) % GROUPS
        placed = jnp.concatenate([hot_group[None], jax.random.permutation(keys_four[1], others).astype(jnp.int32)])
        bounds = jnp.cumsum(quotas).astype(jnp.int32)
        ranks = jnp.arange(TOK_DEV, dtype=jnp.int32)
        position = jnp.searchsorted(bounds, ranks, side='right').astype(jnp.int32)
        within = ranks - (bounds[position] - quotas[position])
        inner_keys = jax.random.split(keys_four[2], GROUPS)
        inner_order = jax.vmap(lambda inner_key: jax.random.permutation(inner_key, GSIZE))(inner_keys).astype(jnp.int32)
        first_pick = inner_order[position, within % GSIZE]
        second_pick = inner_order[position, (within + 1) % GSIZE]
        expert_ids = placed[position][:, None] * GSIZE + jnp.stack([first_pick, second_pick], axis=1)
        order = jax.random.permutation(keys_four[3], TOK_DEV)
        return expert_ids[order].astype(jnp.int32)
    return jax.vmap(one_device)(device_keys, device_ids).reshape(TOKENS, TOPK)


def shard_levels(stream_key, extent, shards, least, top_value):
    def one(dim, parts):
        heights = jax.random.uniform(jax.random.fold_in(jax.random.fold_in(stream_key, 6), dim), (parts,), jnp.float32, least / len(shards), top_value / len(shards))
        return jnp.repeat(jnp.exp(heights), extent[dim] // parts).reshape((-1,) + (1,) * (len(extent) - dim - 1))

    factor_of = one(*shards[0])
    for cut in shards[1:]:
        factor_of = factor_of * one(*cut)
    return factor_of


def normal_values(stream_key, extent, deviation, bound, shards=(), held_as=jnp.bfloat16):
    gain = shard_levels(stream_key, extent, shards, -0.22, 0.18) if shards else 1.0
    result = jax.random.normal(stream_key, extent, jnp.float32) * deviation * gain
    return jnp.minimum(jnp.maximum(result, -bound), bound).astype(held_as)


def setup_inputs(seed: int = 0) -> dict:
    key_list = jax.random.split(jax.random.key(seed), 8)
    tokens = normal_values(key_list[0], (TOKENS, D), 1.0, 6.0, ((0, 8), (1, 4)))
    cotangent = normal_values(key_list[1], (TOKENS, D), 1.0, 6.0, ((0, 8), (1, 4)))
    experts = draw_experts(jax.random.fold_in(key_list[7], 71), 0)
    combine = jnp.clip(0.2 + 0.8 * jax.random.uniform(key_list[3], (TOKENS, TOPK), jnp.float32) ** shard_levels(key_list[3], (TOKENS, TOPK), ((0, 8),), -0.2, 0.2), 0.2, 1.0)
    w_gate = normal_values(key_list[4], (EXPERTS, D, FE), D ** -0.5, 0.125, ((0, 8), (1, 4)))
    w_up = normal_values(key_list[5], (EXPERTS, D, FE), D ** -0.5, 0.125, ((0, 8), (1, 4)))
    w_down = normal_values(key_list[6], (EXPERTS, FE, D), FE ** -0.5, 0.375, ((0, 8), (2, 4)))
    return dict(tokens=tokens, cotangent=cotangent, experts=experts, combine=combine, w_gate=w_gate, w_up=w_up, w_down=w_down)


def slot_table(experts):
    routed = experts.reshape(N_EP, TOK_DEV * TOPK).astype(jnp.int32)
    onehot = (routed[:, :, None] == jnp.arange(EXPERTS, dtype=jnp.int32)[None, None, :]).astype(jnp.int32)
    earlier = jnp.sum((jnp.cumsum(onehot, axis=1) - onehot) * onehot, axis=2).astype(jnp.int32)
    position = jnp.arange(N_EP, dtype=jnp.int32)[:, None] * CAP + earlier
    assigned = jnp.arange(TOKENS * TOPK, dtype=jnp.int32).reshape(N_EP, TOK_DEV * TOPK)
    table = jnp.full((EXPERTS, N_EP * CAP), -1, jnp.int32)
    return table.at[routed, position].set(assigned)


def block_sum(partial_sum):
    rounded = lax.optimization_barrier(partial_sum.astype(jnp.bfloat16)).astype(jnp.float32)
    return jnp.sum(rounded, axis=1)


def reference(tokens, cotangent, experts, combine, w_gate, w_up, w_down):
    table = slot_table(experts)
    weight_flat = lax.optimization_barrier(combine.astype(jnp.bfloat16)).astype(jnp.float32).reshape(-1)
    width_block = D // N_TP
    highest = lax.Precision.HIGHEST

    def per_expert(running, inputs):
        grad_acc, comb_acc = running
        row_ids, gate_mat, up_mat, down_mat = inputs
        filled = row_ids >= 0
        source = jnp.maximum(row_ids, 0)
        token_ids = (source // TOPK).astype(jnp.int32)
        filled_col = filled[:, None]
        rows = jnp.where(filled_col, tokens[token_ids], jnp.zeros((), jnp.bfloat16))
        cots = jnp.where(filled_col, cotangent[token_ids], jnp.zeros((), jnp.bfloat16))
        weights = jnp.where(filled, weight_flat[source], jnp.float32(0.0))[:, None]
        rows_split = rows.astype(jnp.float32).reshape(-1, N_TP, width_block)
        cots_split = cots.astype(jnp.float32).reshape(-1, N_TP, width_block)
        gate_blocks = gate_mat.astype(jnp.float32).reshape(N_TP, width_block, FE)
        up_blocks = up_mat.astype(jnp.float32).reshape(N_TP, width_block, FE)
        down_blocks = down_mat.astype(jnp.float32).reshape(FE, N_TP, width_block)
        gate_pre = block_sum(jnp.einsum('rjd,jdf->rjf', rows_split, gate_blocks, precision=highest))
        up_pre = block_sum(jnp.einsum('rjd,jdf->rjf', rows_split, up_blocks, precision=highest))
        grad_scaled = block_sum(jnp.einsum('rjd,fjd->rjf', cots_split, down_blocks, precision=highest))
        sigmoid_val = jax.nn.sigmoid(gate_pre)
        silu_val = gate_pre * sigmoid_val
        hidden = silu_val * up_pre
        scaled = (weights * hidden).astype(jnp.bfloat16)
        comb_part = jnp.sum(hidden * grad_scaled, axis=1)
        grad_hidden = weights * grad_scaled
        grad_gate_pre = (grad_hidden * up_pre * sigmoid_val * (1.0 + gate_pre * (1.0 - sigmoid_val))).astype(jnp.bfloat16)
        grad_up_pre = (grad_hidden * silu_val).astype(jnp.bfloat16)
        down_grad = jnp.dot(scaled.T, cots, preferred_element_type=jnp.float32)
        gate_grad = jnp.dot(rows.T, grad_gate_pre, preferred_element_type=jnp.float32)
        up_grad = jnp.dot(rows.T, grad_up_pre, preferred_element_type=jnp.float32)
        slot_grad = (jnp.dot(grad_gate_pre, gate_mat.T, preferred_element_type=jnp.float32) + jnp.dot(grad_up_pre, up_mat.T, preferred_element_type=jnp.float32)).astype(jnp.bfloat16)
        grad_acc = grad_acc.at[token_ids].add(jnp.where(filled_col, slot_grad.astype(jnp.float32), jnp.float32(0.0)))
        comb_acc = comb_acc.at[source].add(jnp.where(filled, comb_part, jnp.float32(0.0)))
        return (grad_acc, comb_acc), (gate_grad, up_grad, down_grad)

    start_carry = (jnp.zeros((TOKENS, D), jnp.float32), jnp.zeros((TOKENS * TOPK,), jnp.float32))
    (grad_acc, comb_acc), (gate_grad, up_grad, down_grad) = lax.scan(per_expert, start_carry, (table, w_gate, w_up, w_down))
    return grad_acc.astype(jnp.bfloat16), comb_acc.reshape(TOKENS, TOPK), gate_grad, up_grad, down_grad
```

```python
import functools

import jax
import jax.numpy as jnp
from jax import lax
from jax.experimental import pallas as pl
from jax.experimental.pallas import tpu as pltpu
from jax.sharding import PartitionSpec as P


def slot_positions(routed, total_experts, capacity):
    onehot = (routed[:, None] == jnp.arange(total_experts, dtype=jnp.int32)[None, :]).astype(
        jnp.int32
    )
    earlier = jnp.sum((jnp.cumsum(onehot, axis=0) - onehot) * onehot, axis=1)
    return routed * capacity + earlier


def activation(gate_pre, up_pre, grad_scaled, weight_grid):
    sigmoid_val = jax.nn.sigmoid(gate_pre)
    silu_val = gate_pre * sigmoid_val
    hidden = silu_val * up_pre
    scaled = (weight_grid * hidden).astype(jnp.bfloat16)
    comb_part = jnp.sum(hidden * grad_scaled, axis=3)
    grad_hidden = weight_grid * grad_scaled
    grad_gate_pre = (
        grad_hidden * up_pre * sigmoid_val * (1.0 + gate_pre * (1.0 - sigmoid_val))
    ).astype(jnp.bfloat16)
    grad_up_pre = (grad_hidden * silu_val).astype(jnp.bfloat16)
    return (scaled, grad_gate_pre, grad_up_pre, comb_part)


def body(tokens, cotangent, experts, combine, w_gate, w_up, w_down):
    peers = lax.axis_size("ep")
    local_experts = w_gate.shape[0]
    total_experts = local_experts * peers
    tok_count = tokens.shape[0]
    picks = experts.shape[1]
    assigns = tok_count * picks
    capacity = 2 * assigns // total_experts
    per_peer = local_experts * capacity
    block_width = tokens.shape[1]
    slot_index = slot_positions(experts.reshape(assigns), total_experts, capacity)
    slot_owner = (
        jnp.zeros((total_experts * capacity,), jnp.int32)
        .at[slot_index]
        .set(jnp.arange(assigns, dtype=jnp.int32) + 1)
    )
    filled = slot_owner > 0
    source = jnp.maximum(slot_owner - 1, 0)
    token_ids = source // picks
    filled_col = filled[:, None]
    send_rows = jnp.where(
        filled_col, jnp.take(tokens, token_ids, axis=0), jnp.zeros((), jnp.bfloat16)
    ).reshape(peers, per_peer, block_width)
    send_cots = jnp.where(
        filled_col, jnp.take(cotangent, token_ids, axis=0), jnp.zeros((), jnp.bfloat16)
    ).reshape(peers, per_peer, block_width)
    send_weights = (
        jnp.where(filled, jnp.take(combine.reshape(assigns), source), jnp.float32(0.0))
        .astype(jnp.bfloat16)
        .reshape(peers, per_peer)
    )
    recv_rows, recv_cots, recv_weights = (
        lax.all_to_all(send_rows, "ep", split_axis=0, concat_axis=0, tiled=True),
        lax.all_to_all(send_cots, "ep", split_axis=0, concat_axis=0, tiled=True),
        lax.all_to_all(send_weights, "ep", split_axis=0, concat_axis=0, tiled=True),
    )
    rows_grid = recv_rows.reshape(peers, local_experts, capacity, block_width)
    cots_grid = recv_cots.reshape(peers, local_experts, capacity, block_width)
    weight_grid = recv_weights.astype(jnp.float32).reshape(peers, local_experts, capacity, 1)
    gate_part = jnp.einsum(
        "secd,edf->secf", rows_grid, w_gate, preferred_element_type=jnp.float32
    ).astype(jnp.bfloat16)
    up_part = jnp.einsum(
        "secd,edf->secf", rows_grid, w_up, preferred_element_type=jnp.float32
    ).astype(jnp.bfloat16)
    down_part = jnp.einsum(
        "secd,efd->secf", cots_grid, w_down, preferred_element_type=jnp.float32
    ).astype(jnp.bfloat16)
    gate_pre, up_pre, grad_scaled = (
        lax.psum(gate_part, "tp").astype(jnp.float32),
        lax.psum(up_part, "tp").astype(jnp.float32),
        lax.psum(down_part, "tp").astype(jnp.float32),
    )
    scaled, grad_gate_pre, grad_up_pre, comb_part = activation(
        gate_pre, up_pre, grad_scaled, weight_grid
    )
    down_grad = jnp.einsum("secf,secd->efd", scaled, cots_grid, preferred_element_type=jnp.float32)
    gate_grad = jnp.einsum(
        "secd,secf->edf", rows_grid, grad_gate_pre, preferred_element_type=jnp.float32
    )
    up_grad = jnp.einsum(
        "secd,secf->edf", rows_grid, grad_up_pre, preferred_element_type=jnp.float32
    )
    slot_sum = jnp.einsum(
        "secf,edf->secd", grad_gate_pre, w_gate, preferred_element_type=jnp.float32
    )
    slot_sum = slot_sum + jnp.einsum(
        "secf,edf->secd", grad_up_pre, w_up, preferred_element_type=jnp.float32
    )
    slot_grad = slot_sum.astype(jnp.bfloat16).reshape(peers, per_peer, block_width)
    returned = lax.all_to_all(slot_grad, "ep", split_axis=0, concat_axis=0, tiled=True)
    comb_back = lax.all_to_all(
        comb_part.reshape(peers, per_peer), "ep", split_axis=0, concat_axis=0, tiled=True
    )
    full_grad = returned.reshape(total_experts * capacity, block_width)
    per_assign = (
        jnp.take(full_grad, slot_index, axis=0)
        .astype(jnp.float32)
        .reshape(tok_count, picks, block_width)
    )
    grad_tokens = jnp.sum(per_assign, axis=1).astype(jnp.bfloat16)
    grad_combine = jnp.take(comb_back.reshape(total_experts * capacity), slot_index).reshape(
        tok_count, picks
    )
    return (grad_tokens, grad_combine, gate_grad, up_grad, down_grad)


MESH = pl.DeviceIdType.MESH
LANES = 128


def flip(index, mask, count):
    result, bit = 0, 1
    while bit < count:
        digit = lax.rem(lax.div(index, bit), 2)
        result = result + bit * ((1 - digit) if mask & bit else digit)
        bit *= 2
    return result


def dot(a, b, ca, cb):
    return lax.dot_general(a, b, (((ca,), (cb,)), ((), ())), preferred_element_type=jnp.float32)


def slot_table(first_expert, second_expert, base, slots, cap):
    count = first_expert.shape[1]
    row = lax.broadcasted_iota(jnp.int32, (slots, count), 0)
    expert = base + lax.shift_right_logical(row, cap.bit_length() - 1)
    number = jnp.bitwise_and(row, cap - 1).astype(jnp.float32)
    first = jnp.where(first_expert == expert, 1.0, 0.0)
    second = jnp.where(second_expert == expert, 1.0, 0.0)
    earlier = jnp.where(
        lax.broadcasted_iota(jnp.int32, (count, count), 0)
        < lax.broadcasted_iota(jnp.int32, (count, count), 1), 1.0, 0.0
    ).astype(jnp.bfloat16)
    position = dot((first + second).astype(jnp.bfloat16), earlier, 1, 0)
    here = jnp.where(position == number, 1.0, 0.0)
    return first * here, second * here


def fused_kernel(
    peers, parts, tokens_hbm, cotangent_hbm, experts_hbm, combine_hbm, gate_hbm, up_hbm, down_hbm,
    grad_tokens, grad_combine, gate_grad, up_grad, down_grad,
    tokens, cotangent, experts, combine, w_gate, w_up, w_down,
    send_t, send_c, cross_t, cross_c, cross_e, relay_t, relay_c, recv_t, recv_c,
    wsend, wrecv, part_t, part_c, core_t, core_c, pair_t, pair_c, pair_in_t, pair_in_c,
    acts, comb, slot, ret,
    comb_ret, gather, gather_relay, onehot_k,
    sem_in, sem_t, sem_c, sem_rt, sem_rc, sem_xt, sem_xc, sem_w, sem_e,
    sem_core, sem_pair, sem_act, sem_comb, sem_ret, sem_cret,
):
    ep, tp = lax.axis_index("ep"), lax.axis_index("tp")
    core = lax.rem(tp, 2)
    mate = tp + 1 - 2 * core
    across = lax.rem(tp + 2, parts)
    f = w_gate.shape[1]
    slots = recv_t.shape[0]
    cap = slots // peers
    half = peers // 2
    per_row = LANES // cap
    side_of, place = lax.div(ep, half), lax.rem(ep, half)
    peer = [flip(ep, d, peers) for d in range(peers)]
    spot = [lax.rem(p, half) for p in peer]
    layer, column = lax.div(ep, 2), lax.rem(ep, 2)
    inner = jnp.where(layer == 1 + side_of, 1, 0)
    is_inner, is_outer = inner == 1, inner == 0
    layers = (layer, layer + 1 - 2 * lax.rem(layer, 2), 2 - side_of, 3 * (1 - side_of))
    far_gate = (2 * layers[2] + column, tp)

    def block(index, size=cap):
        return pl.ds(pl.multiple_of(index * size, size), size)

    def remote(src, dst, sems, index, device):
        return pltpu.make_async_remote_copy(
            src_ref=src, dst_ref=dst, send_sem=sems.at[0, index], recv_sem=sems.at[1, index],
            device_id=device, device_id_type=MESH,
        )

    loads = [
        pltpu.make_async_copy(source, target, sem_in.at[i])
        for i, (source, target) in enumerate((
            (experts_hbm, experts), (combine_hbm, combine), (tokens_hbm, tokens),
            (cotangent_hbm, cotangent), (gate_hbm.at[0], w_gate), (up_hbm.at[0], w_up),
            (down_hbm.at[0], w_down),
        ))
    ]
    for load in loads:
        load.start()
    barrier = pltpu.get_barrier_semaphore()
    for d in range(1, peers):
        pl.semaphore_signal(barrier, inc=1, device_id=(peer[d], tp), device_id_type=MESH)
    pl.semaphore_signal(barrier, inc=1, device_id=(ep, mate), device_id_type=MESH)
    pl.semaphore_signal(barrier, inc=1, device_id=(ep, across), device_id_type=MESH)
    loads[0].wait()
    loads[1].wait()

    first, second = slot_table(experts[0:1], experts[1:2], 0, slots, cap)
    onehot_k[0] = first
    onehot_k[1] = second
    gather[...] = (first + second).astype(jnp.bfloat16)
    weight = combine[...].astype(jnp.bfloat16).astype(jnp.float32)
    weight_column = jnp.sum(first * weight[0:1] + second * weight[1:2], axis=1, keepdims=True)
    for q in range(slots // LANES):
        wide = jnp.broadcast_to(weight_column[q * LANES:(q + 1) * LANES], (LANES, LANES))
        wsend[q] = wide.T[:8]
    wrecv[ep] = wsend[lax.div(ep, per_row)]
    loads[2].wait()
    loads[3].wait()
    with jax.named_scope("barrier"):
        pl.semaphore_wait(barrier, peers + 1)

    own = gather[block(side_of, half * cap)]
    send_e = remote(experts, cross_e.at[1 - inner], sem_e, 1 - inner, far_gate)
    send_e.start()
    copy_w = {}
    for d in range(1, peers):
        copy_w[d] = remote(
            wsend.at[lax.div(peer[d], per_row)], wrecv.at[ep], sem_w, d, (peer[d], tp)
        )
        copy_w[d].start()
    raw_t = remote(tokens, cross_t.at[1 - inner], sem_xt, 1 - inner, far_gate)
    raw_c = remote(cotangent, cross_c.at[1 - inner], sem_xc, 1 - inner, far_gate)

    raw_t.start()
    raw_c.start()

    def near_copy(d, packed, landed, sems):
        return remote(packed.at[block(spot[d])], landed.at[block(ep)], sems, d, (peer[d], tp))

    for source, packed, landed, sems in (
        (tokens, send_t, recv_t, sem_t), (cotangent, send_c, recv_c, sem_c)
    ):
        packed[...] = dot(own, source[...], 1, 0).astype(jnp.bfloat16)
        for d in (1, 2, 3):
            near_copy(d, packed, landed, sems).start()
        landed[block(ep)] = packed[block(place)]

    for load in loads[4:]:
        load.wait()

    def relay_copy(k, d, packed, landed, sems):
        return remote(
            packed.at[k, block(spot[d])], landed.at[block(2 * layers[2 + k] + column)],
            sems, 4 * k + d, (peer[d], tp),
        )

    def relay_table(k):
        remote(experts, cross_e.at[k], sem_e, k, far_gate).wait_recv()
        chosen_a, chosen_b = slot_table(
            cross_e[k, 0:1], cross_e[k, 1:2], side_of * half, half * cap, cap
        )
        gather_relay[k] = (chosen_a + chosen_b).astype(jnp.bfloat16)

    def relay(k, source, crossed, packed, landed, sems_in, sems_out):
        with jax.named_scope("wait_raw"):
            remote(source, crossed.at[k], sems_in, k, far_gate).wait_recv()
        packed[k] = dot(gather_relay[k], crossed[k], 1, 0).astype(jnp.bfloat16)
        for d in (2, 3, 1):
            relay_copy(k, d, packed, landed, sems_out).start()
        landed[block(2 * layers[2 + k] + column)] = packed[k, block(place)]

    def relay_tokens(k, gate):
        relay(k, tokens, cross_t, relay_t, recv_t, sem_xt, sem_rt)

    def relay_cots(k, gate):
        relay(k, cotangent, cross_c, relay_c, recv_c, sem_xc, sem_rc)

    def arrive(j, gate, packed, relayed, landed, near_sems, sems):
        if j < 2:
            for d in (2 * j, 2 * j + 1):
                if d:
                    near_copy(d, packed, landed, near_sems).wait_recv()
        else:
            for d in (1,) if gate else (2, 3):
                with jax.named_scope("arrive%d" % d):
                    relay_copy(j - 2, d, relayed, landed, sems).wait_recv()

    pairs = peers // 2

    def core_copy(i):
        part, landed = (part_t, core_t) if i < pairs else (part_c, core_c)
        j = i % pairs
        return remote(part.at[j, block(1 - core)], landed.at[j], sem_core, i, (ep, mate))

    def pair_copy(i):
        summed, landed = (pair_t, pair_in_t) if i < pairs else (pair_c, pair_in_c)
        return remote(summed.at[i % pairs], landed.at[i % pairs], sem_pair, i, (ep, across))

    def act_copy(j):
        rows = block(2 * layers[j] + core)
        return remote(acts.at[rows], acts.at[rows], sem_act, j, (ep, mate))

    def comb_copy(j):
        source = 2 * layers[j] + core
        return remote(comb.at[source], comb.at[source], sem_comb, j, (ep, mate))

    def distance(j, b):
        return 2 * j + b if j < 2 else 4 + 2 * lax.rem(j + inner, 2) + b

    def back_copies(j, b):
        target = 2 * layers[j] + lax.rem(column + b, 2)
        return (
            remote(
                slot.at[block(target)], ret.at[block(ep)], sem_ret, distance(j, b), (target, tp)
            ),
            remote(comb.at[target], comb_ret.at[ep], sem_cret, distance(j, b), (target, tp)),
        )

    def parts_tokens(j, gate):
        arrive(j, gate, send_t, relay_t, recv_t, sem_t, sem_rt)
        rows = recv_t[block(layers[j], 2 * cap)]
        part_t[j, :, :f] = dot(rows, w_gate[...], 1, 0).astype(jnp.bfloat16)
        part_t[j, :, f:] = dot(rows, w_up[...], 1, 0).astype(jnp.bfloat16)
        core_copy(j).start()

    def parts_cots(j, gate):
        arrive(j, gate, send_c, relay_c, recv_c, sem_c, sem_rc)
        cots = recv_c[block(layers[j], 2 * cap)]
        part_c[j] = dot(cots, w_down[...], 1, 1).astype(jnp.bfloat16)
        core_copy(pairs + j).start()

    def pair_sum(j, i, part, landed, summed):
        core_copy(i).wait_recv()
        mine = part[j, block(core)].astype(jnp.float32)
        summed[j] = (mine + landed[j].astype(jnp.float32)).astype(jnp.bfloat16)
        pair_copy(i).start()

    def pair_tokens(j, gate):
        pair_sum(j, j, part_t, core_t, pair_t)

    def pair_cots(j, gate):
        pair_sum(j, pairs + j, part_c, core_c, pair_c)

    def act(j, gate):
        if j == 0:
            for d in range(1, peers):
                copy_w[d].wait_recv()
        pair_copy(j).wait_recv()
        pair_copy(pairs + j).wait_recv()
        source = 2 * layers[j] + core
        gate_pre = pair_t[j, :, :f].astype(jnp.float32) + pair_in_t[j, :, :f].astype(jnp.float32)
        up_pre = pair_t[j, :, f:].astype(jnp.float32) + pair_in_t[j, :, f:].astype(jnp.float32)
        grad_scaled = pair_c[j].astype(jnp.float32) + pair_in_c[j].astype(jnp.float32)
        weights = jnp.broadcast_to(wrecv[source][0:1], (LANES, LANES)).T
        w = weights[:cap]
        for r in range(1, per_row):
            w = jnp.where(lax.rem(ep, per_row) == r, weights[r * cap:(r + 1) * cap], w)
        w = w[:, 0:1]
        sigmoid = jax.nn.sigmoid(gate_pre)
        silu = gate_pre * sigmoid
        hidden = silu * up_pre
        grad_hidden = w * grad_scaled
        rows = block(source)
        acts[rows, :f] = (w * hidden).astype(jnp.bfloat16)
        acts[rows, f:2 * f] = (
            grad_hidden * up_pre * sigmoid * (1.0 + gate_pre * (1.0 - sigmoid))
        ).astype(jnp.bfloat16)
        acts[rows, 2 * f:] = (grad_hidden * silu).astype(jnp.bfloat16)
        act_copy(j).start()
        total = jnp.sum(hidden * grad_scaled, axis=1, keepdims=True)
        wide = jnp.concatenate([jnp.broadcast_to(total, (cap, LANES))] * per_row, axis=0)
        comb[source] = wide.T[:8]
        comb_copy(j).start()

    def slots_back(j, gate):
        act_copy(j).wait_recv()
        comb_copy(j).wait_recv()
        rows = block(layers[j], 2 * cap)
        value = dot(acts[rows, f:2 * f], w_gate[...], 1, 1) + dot(acts[rows, 2 * f:], w_up[...], 1, 1)
        slot[rows] = value.astype(jnp.bfloat16)
        for b in range(2):
            if j == b == 0:
                ret[block(ep)] = slot[block(ep)]
                comb_ret[ep] = comb[ep]
            else:
                for copy in back_copies(j, b):
                    copy.start()

    def tables(k, gate):
        relay_table(k)

    def grads(which, gate):
        if which == 0:
            down_grad[...] = dot(acts[:, :f], recv_c[...], 0, 0)
        elif which == 1:
            gate_grad[...] = dot(recv_t[...], acts[:, f:2 * f], 0, 0)
        else:
            up_grad[...] = dot(recv_t[...], acts[:, 2 * f:], 0, 0)

    names = {
        "T": tables, "rt": relay_tokens, "rc": relay_cots, "pt": parts_tokens, "pc": parts_cots,
        "st": pair_tokens, "sc": pair_cots, "a": act, "b": slots_back, "g": grads,
    }
    outer_order = (
        "pt0", "pc0", "st0", "sc0", "pt1", "st1", "pc1", "sc1", "a0", "b0", "pt3", "st3",
        "a1", "b1", "pc3", "sc3", "pt2", "st2", "a3", "b3", "pc2", "sc2", "a2", "b2",
    )
    inner_order = (
        "pt0", "T1", "pc0", "st0", "T0", "sc0", "rt1", "a0", "rc1", "b0", "pt3", "st3",
        "rt0", "pt1", "st1", "pc3", "sc3", "rc0", "pc1", "sc1", "a3", "pt2", "st2", "a1",
        "b3", "b1", "pc2", "sc2", "a2", "b2",
    )
    for role, order, gate in ((is_outer, outer_order, False), (is_inner, inner_order, True)):
        @pl.when(role)
        def _():
            for word in order:
                with jax.named_scope(word):
                    names[word[:-1]](int(word[-1]), gate)

    for which in range(3):
        with jax.named_scope("g%d" % which):
            grads(which, None)

    with jax.named_scope("cret"):
        for d in range(1, peers):
            remote(comb.at[0], comb_ret.at[0], sem_cret, d, (peer[d], tp)).wait_recv()
    part_lane = lax.broadcasted_iota(jnp.int32, (1, LANES), 1)
    totals = [jnp.zeros((1, tokens.shape[0]), jnp.float32)] * 2
    for q in range(slots // LANES):
        row = comb_ret[q * per_row][0:1]
        for r in range(1, per_row):
            row = jnp.where(part_lane >= r * cap, comb_ret[q * per_row + r][0:1], row)
        values = jnp.broadcast_to(row, (LANES, LANES)).T[:, 0:1]
        for k in range(2):
            chosen = onehot_k[k, q * LANES:(q + 1) * LANES] * values
            totals[k] = totals[k] + jnp.sum(chosen, axis=0, keepdims=True)
    for k in range(2):
        grad_combine[k:k + 1] = totals[k]
    with jax.named_scope("ret"):
        for d in range(1, peers):
            remote(slot.at[block(0)], ret.at[block(0)], sem_ret, d, (peer[d], tp)).wait_recv()
    grad_tokens[...] = dot(gather[...], ret[...], 0, 0).astype(jnp.bfloat16)
    for copy in (send_e, raw_t, raw_c, *copy_w.values()):
        copy.wait_send()
    for d in range(1, half):
        near_copy(d, send_t, recv_t, sem_t).wait_send()
        near_copy(d, send_c, recv_c, sem_c).wait_send()
    for j in range(pairs):
        for copy in (
            core_copy(j), core_copy(pairs + j), pair_copy(j), pair_copy(pairs + j),
            act_copy(j), comb_copy(j),
        ):
            copy.wait_send()
        for b in range(2):
            if j or b:
                for copy in back_copies(j, b):
                    copy.wait_send()

    @pl.when(is_inner)
    def _():
        for k in range(2):
            for d in range(1, half):
                relay_copy(k, d, relay_t, recv_t, sem_rt).wait_send()
                relay_copy(k, d, relay_c, recv_c, sem_rc).wait_send()


def store_kernel(count, *refs):
    sources, targets, sems = refs[:count], refs[count:2 * count], refs[2 * count]
    copies = [
        pltpu.make_async_copy(source, target, sems.at[i])
        for i, (source, target) in enumerate(zip(sources, targets))
    ]
    for copy in copies:
        copy.start()
    for copy in copies:
        copy.wait()


def fused_body(peers, parts, tokens, cotangent, experts, combine, w_gate, w_up, w_down):
    count, width = tokens.shape
    f = w_gate.shape[2]
    picks = experts.shape[1]
    cap = 2 * count * picks // peers
    slots = peers * cap
    pairs = peers // 2
    bf16, f32 = jnp.bfloat16, jnp.float32
    dma = pltpu.SemaphoreType.DMA
    vmem = pl.BlockSpec(memory_space=pltpu.VMEM)
    hbm = pl.BlockSpec(memory_space=pltpu.HBM)
    shapes = (
        jax.ShapeDtypeStruct((count, width), bf16),
        jax.ShapeDtypeStruct((picks, count), f32),
        jax.ShapeDtypeStruct((width, f), f32),
        jax.ShapeDtypeStruct((width, f), f32),
        jax.ShapeDtypeStruct((f, width), f32),
    )
    half_rows = pltpu.VMEM((slots // 2, width), bf16)
    relayed = pltpu.VMEM((2, slots // 2, width), bf16)
    rows = pltpu.VMEM((count, width), bf16)
    crossed = pltpu.VMEM((2, count, width), bf16)
    landed = pltpu.VMEM((slots, width), bf16)
    sums_t = pltpu.VMEM((pairs, cap, 2 * f), bf16)
    sums_c = pltpu.VMEM((pairs, cap, f), bf16)
    small = pltpu.VMEM((peers, 8, LANES), f32)
    outs = pl.pallas_call(
        functools.partial(fused_kernel, peers, parts),
        out_shape=shapes,
        in_specs=[hbm] * 7,
        out_specs=(vmem,) * 5,
        scratch_shapes=[
            rows, rows, pltpu.VMEM((picks, count), jnp.int32), pltpu.VMEM((picks, count), f32),
            pltpu.VMEM((width, f), bf16), pltpu.VMEM((width, f), bf16), pltpu.VMEM((f, width), bf16),
            half_rows, half_rows, crossed, crossed, pltpu.VMEM((2, picks, count), jnp.int32),
            relayed, relayed, landed, landed,
            pltpu.VMEM((slots // LANES, 8, LANES), f32), small,
            pltpu.VMEM((pairs, 2 * cap, 2 * f), bf16), pltpu.VMEM((pairs, 2 * cap, f), bf16),
            sums_t, sums_c, sums_t, sums_c, sums_t, sums_c,
            pltpu.VMEM((slots, 3 * f), bf16), small, landed, landed,
            small, pltpu.VMEM((slots, count), bf16), pltpu.VMEM((2, slots // 2, count), bf16),
            pltpu.VMEM((picks, slots, count), f32),
            dma((7,)), dma((2, peers)), dma((2, peers)), dma((2, peers)), dma((2, peers)),
            dma((2, 2)), dma((2, 2)), dma((2, peers)), dma((2, 2)),
            dma((2, 2 * pairs)), dma((2, 2 * pairs)), dma((2, pairs)), dma((2, pairs)),
            dma((2, peers)), dma((2, peers)),
        ],
        compiler_params=pltpu.CompilerParams(
            collective_id=0, has_side_effects=True, vmem_limit_bytes=48 * 1024 * 1024
        ),
    )(*(
        pltpu.with_memory_space_constraint(x, pltpu.HBM)
        for x in (tokens, cotangent, experts.T, combine.T, w_gate, w_up, w_down)
    ))
    outs = pl.pallas_call(
        functools.partial(store_kernel, len(outs)),
        out_shape=shapes,
        in_specs=[vmem] * 5,
        out_specs=(hbm,) * 5,
        scratch_shapes=[dma((5,))],
        compiler_params=pltpu.CompilerParams(vmem_limit_bytes=1024 * 1024),
    )(*outs)
    return outs[0], outs[1].T, outs[2][None], outs[3][None], outs[4][None]


def choose(mesh, tokens, cotangent, experts, combine, w_gate, w_up, w_down):
    peers, parts = mesh.shape["ep"], mesh.shape["tp"]
    count, width = tokens.shape
    cap = 2 * count * experts.shape[1] // w_gate.shape[0] // peers
    fits = (
        w_gate.shape[0] == 1 and experts.shape[1] == 2 and parts == 4
        and peers == 8 and cap in (16, 32, 64, 128)
        and count % LANES == 0 and width % LANES == 0
        and w_gate.shape[2] % LANES == 0 and peers * cap % LANES == 0
    )
    run = functools.partial(fused_body, peers, parts) if fits else body
    return run(tokens, cotangent, experts, combine, w_gate, w_up, w_down)


def solution(mesh):
    return jax.shard_map(
        functools.partial(choose, mesh),
        mesh=mesh,
        in_specs=(
            P("ep", "tp"),
            P("ep", "tp"),
            P("ep", None),
            P("ep", None),
            P("ep", "tp", None),
            P("ep", "tp", None),
            P("ep", None, "tp"),
        ),
        out_specs=(
            P("ep", "tp"),
            P("ep", None),
            P("ep", "tp", None),
            P("ep", "tp", None),
            P("ep", None, "tp"),
        ),
        check_vma=False,
    )
```

```python
import functools

import jax
import jax.numpy as jnp
from jax import lax
from jax.experimental import pallas as pl
from jax.experimental.pallas import tpu as pltpu
from jax.sharding import PartitionSpec as P


def slot_positions(routed, total_experts, capacity):
    onehot = (routed[:, None] == jnp.arange(total_experts, dtype=jnp.int32)[None, :]).astype(
        jnp.int32
    )
    earlier = jnp.sum((jnp.cumsum(onehot, axis=0) - onehot) * onehot, axis=1)
    return routed * capacity + earlier


def activation(gate_pre, up_pre, grad_scaled, weight_grid):
    sigmoid_val = jax.nn.sigmoid(gate_pre)
    silu_val = gate_pre * sigmoid_val
    hidden = silu_val * up_pre
    scaled = (weight_grid * hidden).astype(jnp.bfloat16)
    comb_part = jnp.sum(hidden * grad_scaled, axis=3)
    grad_hidden = weight_grid * grad_scaled
    grad_gate_pre = (
        grad_hidden * up_pre * sigmoid_val * (1.0 + gate_pre * (1.0 - sigmoid_val))
    ).astype(jnp.bfloat16)
    grad_up_pre = (grad_hidden * silu_val).astype(jnp.bfloat16)
    return (scaled, grad_gate_pre, grad_up_pre, comb_part)


def body(tokens, cotangent, experts, combine, w_gate, w_up, w_down):
    peers = lax.axis_size("ep")
    local_experts = w_gate.shape[0]
    total_experts = local_experts * peers
    tok_count = tokens.shape[0]
    picks = experts.shape[1]
    assigns = tok_count * picks
    capacity = 2 * assigns // total_experts
    per_peer = local_experts * capacity
    block_width = tokens.shape[1]
    slot_index = slot_positions(experts.reshape(assigns), total_experts, capacity)
    slot_owner = (
        jnp.zeros((total_experts * capacity,), jnp.int32)
        .at[slot_index]
        .set(jnp.arange(assigns, dtype=jnp.int32) + 1)
    )
    filled = slot_owner > 0
    source = jnp.maximum(slot_owner - 1, 0)
    token_ids = source // picks
    filled_col = filled[:, None]
    send_rows = jnp.where(
        filled_col, jnp.take(tokens, token_ids, axis=0), jnp.zeros((), jnp.bfloat16)
    ).reshape(peers, per_peer, block_width)
    send_cots = jnp.where(
        filled_col, jnp.take(cotangent, token_ids, axis=0), jnp.zeros((), jnp.bfloat16)
    ).reshape(peers, per_peer, block_width)
    send_weights = (
        jnp.where(filled, jnp.take(combine.reshape(assigns), source), jnp.float32(0.0))
        .astype(jnp.bfloat16)
        .reshape(peers, per_peer)
    )
    recv_rows, recv_cots, recv_weights = (
        lax.all_to_all(send_rows, "ep", split_axis=0, concat_axis=0, tiled=True),
        lax.all_to_all(send_cots, "ep", split_axis=0, concat_axis=0, tiled=True),
        lax.all_to_all(send_weights, "ep", split_axis=0, concat_axis=0, tiled=True),
    )
    rows_grid = recv_rows.reshape(peers, local_experts, capacity, block_width)
    cots_grid = recv_cots.reshape(peers, local_experts, capacity, block_width)
    weight_grid = recv_weights.astype(jnp.float32).reshape(peers, local_experts, capacity, 1)
    gate_part = jnp.einsum(
        "secd,edf->secf", rows_grid, w_gate, preferred_element_type=jnp.float32
    ).astype(jnp.bfloat16)
    up_part = jnp.einsum(
        "secd,edf->secf", rows_grid, w_up, preferred_element_type=jnp.float32
    ).astype(jnp.bfloat16)
    down_part = jnp.einsum(
        "secd,efd->secf", cots_grid, w_down, preferred_element_type=jnp.float32
    ).astype(jnp.bfloat16)
    gate_pre, up_pre, grad_scaled = (
        lax.psum(gate_part, "tp").astype(jnp.float32),
        lax.psum(up_part, "tp").astype(jnp.float32),
        lax.psum(down_part, "tp").astype(jnp.float32),
    )
    scaled, grad_gate_pre, grad_up_pre, comb_part = activation(
        gate_pre, up_pre, grad_scaled, weight_grid
    )
    down_grad = jnp.einsum("secf,secd->efd", scaled, cots_grid, preferred_element_type=jnp.float32)
    gate_grad = jnp.einsum(
        "secd,secf->edf", rows_grid, grad_gate_pre, preferred_element_type=jnp.float32
    )
    up_grad = jnp.einsum(
        "secd,secf->edf", rows_grid, grad_up_pre, preferred_element_type=jnp.float32
    )
    slot_sum = jnp.einsum(
        "secf,edf->secd", grad_gate_pre, w_gate, preferred_element_type=jnp.float32
    )
    slot_sum = slot_sum + jnp.einsum(
        "secf,edf->secd", grad_up_pre, w_up, preferred_element_type=jnp.float32
    )
    slot_grad = slot_sum.astype(jnp.bfloat16).reshape(peers, per_peer, block_width)
    returned = lax.all_to_all(slot_grad, "ep", split_axis=0, concat_axis=0, tiled=True)
    comb_back = lax.all_to_all(
        comb_part.reshape(peers, per_peer), "ep", split_axis=0, concat_axis=0, tiled=True
    )
    full_grad = returned.reshape(total_experts * capacity, block_width)
    per_assign = (
        jnp.take(full_grad, slot_index, axis=0)
        .astype(jnp.float32)
        .reshape(tok_count, picks, block_width)
    )
    grad_tokens = jnp.sum(per_assign, axis=1).astype(jnp.bfloat16)
    grad_combine = jnp.take(comb_back.reshape(total_experts * capacity), slot_index).reshape(
        tok_count, picks
    )
    return (grad_tokens, grad_combine, gate_grad, up_grad, down_grad)


MESH = pl.DeviceIdType.MESH
LANES = 128


def flip(index, mask, count):
    result, bit = 0, 1
    while bit < count:
        digit = lax.rem(lax.div(index, bit), 2)
        result = result + bit * ((1 - digit) if mask & bit else digit)
        bit *= 2
    return result


def dot(a, b, ca, cb):
    return lax.dot_general(a, b, (((ca,), (cb,)), ((), ())), preferred_element_type=jnp.float32)


def slot_table(first_expert, second_expert, base, slots, cap):
    count = first_expert.shape[1]
    row = lax.broadcasted_iota(jnp.int32, (slots, count), 0)
    expert = base + lax.shift_right_logical(row, cap.bit_length() - 1)
    number = jnp.bitwise_and(row, cap - 1).astype(jnp.float32)
    first = jnp.where(first_expert == expert, 1.0, 0.0)
    second = jnp.where(second_expert == expert, 1.0, 0.0)
    earlier = jnp.where(
        lax.broadcasted_iota(jnp.int32, (count, count), 0)
        < lax.broadcasted_iota(jnp.int32, (count, count), 1), 1.0, 0.0
    ).astype(jnp.bfloat16)
    position = dot((first + second).astype(jnp.bfloat16), earlier, 1, 0)
    here = jnp.where(position == number, 1.0, 0.0)
    return first * here, second * here


def fused_kernel(
    peers, parts, tokens_hbm, cotangent_hbm, experts_hbm, combine_hbm, gate_hbm, up_hbm, down_hbm,
    grad_tokens, grad_combine, gate_grad, up_grad, down_grad,
    tokens, cotangent, experts, combine, w_gate, w_up, w_down,
    send_t, send_c, cross_t, cross_c, cross_e, relay_t, relay_c, recv_t, recv_c,
    wsend, wrecv, part_t, part_c, core_t, core_c, pair_t, pair_c, pair_in_t, pair_in_c,
    acts, comb, slot, ret,
    comb_ret, gather, gather_relay, onehot_k,
    sem_in, sem_t, sem_c, sem_rt, sem_rc, sem_x, sem_w, sem_e,
    sem_core, sem_pair, sem_act, sem_ret, sem_cret,
):
    ep, tp = lax.axis_index("ep"), lax.axis_index("tp")
    core = lax.rem(tp, 2)
    mate = tp + 1 - 2 * core
    across = lax.rem(tp + 2, parts)
    f = w_gate.shape[1]
    slots = recv_t.shape[0]
    cap = slots // peers
    half = peers // 2
    per_row = LANES // cap
    side_of, place = lax.div(ep, half), lax.rem(ep, half)
    peer = [flip(ep, d, peers) for d in range(peers)]
    spot = [lax.rem(p, half) for p in peer]
    layer, column = lax.div(ep, 2), lax.rem(ep, 2)
    inner = jnp.where(layer == 1 + side_of, 1, 0)
    is_inner, is_outer = inner == 1, inner == 0
    layers = (layer, layer + 1 - 2 * lax.rem(layer, 2), 2 - side_of, 3 * (1 - side_of))
    far_gate = (2 * layers[2] + column, tp)

    def block(index, size=cap):
        return pl.ds(pl.multiple_of(index * size, size), size)

    def remote(src, dst, sems, sent, landed, device):
        return pltpu.make_async_remote_copy(
            src_ref=src, dst_ref=dst, send_sem=sems.at[sent], recv_sem=sems.at[landed],
            device_id=device, device_id_type=MESH,
        )

    def wait_sent(ref, sems, sent):
        remote(ref, ref, sems, sent, sent, (ep, mate)).wait_send()

    def wait_landed(ref, sems, landed):
        remote(ref, ref, sems, landed, landed, (ep, mate)).wait_recv()

    loads = [
        pltpu.make_async_copy(source, target, sem_in.at[i])
        for i, (source, target) in enumerate((
            (experts_hbm, experts), (combine_hbm, combine), (tokens_hbm, tokens),
            (cotangent_hbm, cotangent), (gate_hbm.at[0], w_gate), (up_hbm.at[0], w_up),
            (down_hbm.at[0], w_down),
        ))
    ]
    for load in loads:
        load.start()
    barrier = pltpu.get_barrier_semaphore()
    for device in [(peer[d], tp) for d in range(1, half)] + [(ep, mate), (ep, across)]:
        pl.semaphore_signal(barrier, inc=1, device_id=device, device_id_type=MESH)

    @pl.when(is_inner)
    def _():
        for far in (2, 3):
            device = (2 * layers[far] + column, tp)
            pl.semaphore_signal(barrier, inc=1, device_id=device, device_id_type=MESH)

    loads[0].wait()
    loads[1].wait()

    first, second = slot_table(experts[0:1], experts[1:2], 0, slots, cap)
    onehot_k[0] = first
    onehot_k[1] = second
    gather[...] = (first + second).astype(jnp.bfloat16)
    weight = combine[...].astype(jnp.bfloat16).astype(jnp.float32)
    weight_column = jnp.sum(first * weight[0:1] + second * weight[1:2], axis=1, keepdims=True)
    for q in range(slots // LANES):
        wide = jnp.broadcast_to(weight_column[q * LANES:(q + 1) * LANES], (LANES, LANES))
        wsend[q] = wide.T[:8]
    wrecv[ep] = wsend[lax.div(ep, per_row)]
    loads[2].wait()
    loads[3].wait()
    with jax.named_scope("barrier"):
        pl.semaphore_wait(barrier, half + 2)

    own = gather[block(side_of, half * cap)]
    send_e = remote(experts, cross_e.at[1 - inner], sem_e, 2, 1 - inner, far_gate)
    send_e.start()

    def send_weights(target, far):
        remote(
            wsend.at[lax.div(target, per_row)], wrecv.at[ep], sem_w, 2, far, (target, tp)
        ).start()

    for d in range(1, half):
        send_weights(peer[d], 0)
    remote(tokens, cross_t.at[1 - inner], sem_x, 4, 1 - inner, far_gate).start()
    remote(cotangent, cross_c.at[1 - inner], sem_x, 4, 3 - inner, far_gate).start()

    for source, packed, landed, sems in (
        (tokens, send_t, recv_t, sem_t), (cotangent, send_c, recv_c, sem_c)
    ):
        packed[...] = dot(own, source[...], 1, 0).astype(jnp.bfloat16)
        for d in range(1, half):
            remote(
                packed.at[block(spot[d])], landed.at[block(ep)], sems, 2, min(d - 1, 1), (peer[d], tp)
            ).start()
        landed[block(ep)] = packed[block(place)]

    for load in loads[4:]:
        load.wait()

    def relay_table(k):
        wait_landed(cross_e.at[k], sem_e, k)
        chosen_a, chosen_b = slot_table(
            cross_e[k, 0:1], cross_e[k, 1:2], side_of * half, half * cap, cap
        )
        gather_relay[k] = (chosen_a + chosen_b).astype(jnp.bfloat16)

    def relay(k, landed_in, crossed, packed, landed, sems):
        wait_landed(crossed.at[k], sem_x, landed_in)
        packed[k] = dot(gather_relay[k], crossed[k], 1, 0).astype(jnp.bfloat16)
        rows = block(2 * layers[2 + k] + column)
        for d in range(1, half):
            remote(packed.at[k, block(spot[d])], landed.at[rows], sems, 2, k, (peer[d], tp)).start()
        landed[rows] = packed[k, block(place)]

    def relay_tokens(k, gate):
        relay(k, k, cross_t, relay_t, recv_t, sem_rt)

    def relay_cots(k, gate):
        relay(k, 2 + k, cross_c, relay_c, recv_c, sem_rc)

    def arrive(j, gate, landed, near_sems, sems):
        count = cap if j == 0 or (gate and j > 1) else 2 * cap
        wait_landed(landed.at[block(0, count)], sems if j > 1 else near_sems, j % 2)

    def weights_out(k, gate):
        for b in range(2):
            target = 2 * layers[2 + k] + b
            send_weights(target, 1)

    pairs = peers // 2

    def core_copy(i):
        part, landed = (part_t, core_t) if i < pairs else (part_c, core_c)
        j = i % pairs
        return remote(
            part.at[j, block(1 - core)], landed.at[j], sem_core, 2 * pairs + i // pairs, i, (ep, mate)
        )

    def pair_copy(i):
        summed, landed = (pair_t, pair_in_t) if i < pairs else (pair_c, pair_in_c)
        return remote(
            summed.at[i % pairs], landed.at[i % pairs], sem_pair, 2 * pairs + i // pairs, i,
            (ep, across),
        )

    def act_copy(j):
        rows = block(2 * layers[j] + core)
        return remote(acts.at[rows], acts.at[rows], sem_act, pairs, j, (ep, mate))

    def comb_send(source, device):
        remote(comb.at[source], comb_ret.at[ep], sem_cret, 1, 0, (source, device)).start()

    def parts_tokens(j, gate):
        arrive(j, gate, recv_t, sem_t, sem_rt)
        rows = recv_t[block(layers[j], 2 * cap)]
        part_t[j, :, :f] = dot(rows, w_gate[...], 1, 0).astype(jnp.bfloat16)
        part_t[j, :, f:] = dot(rows, w_up[...], 1, 0).astype(jnp.bfloat16)
        core_copy(j).start()

    def parts_cots(j, gate):
        arrive(j, gate, recv_c, sem_c, sem_rc)
        cots = recv_c[block(layers[j], 2 * cap)]
        part_c[j] = dot(cots, w_down[...], 1, 1).astype(jnp.bfloat16)
        core_copy(pairs + j).start()

    def pair_sum(j, i, part, landed, summed):
        core_copy(i).wait_recv()
        mine = part[j, block(core)].astype(jnp.float32)
        summed[j] = (mine + landed[j].astype(jnp.float32)).astype(jnp.bfloat16)
        pair_copy(i).start()

    def pair_tokens(j, gate):
        pair_sum(j, j, part_t, core_t, pair_t)

    def pair_cots(j, gate):
        pair_sum(j, pairs + j, part_c, core_c, pair_c)

    def act(j, gate):
        if j == 0:
            wait_landed(wrecv.at[0:half - 1], sem_w, 0)
        if j == 3:
            wait_landed(wrecv.at[0:half], sem_w, 1)
        pair_copy(j).wait_recv()
        pair_copy(pairs + j).wait_recv()
        source = 2 * layers[j] + core
        gate_pre = pair_t[j, :, :f].astype(jnp.float32) + pair_in_t[j, :, :f].astype(jnp.float32)
        up_pre = pair_t[j, :, f:].astype(jnp.float32) + pair_in_t[j, :, f:].astype(jnp.float32)
        grad_scaled = pair_c[j].astype(jnp.float32) + pair_in_c[j].astype(jnp.float32)
        weights = jnp.broadcast_to(wrecv[source][0:1], (LANES, LANES)).T
        w = weights[:cap]
        for r in range(1, per_row):
            w = jnp.where(lax.rem(ep, per_row) == r, weights[r * cap:(r + 1) * cap], w)
        w = w[:, 0:1]
        sigmoid = jax.nn.sigmoid(gate_pre)
        silu = gate_pre * sigmoid
        hidden = silu * up_pre
        grad_hidden = w * grad_scaled
        rows = block(source)
        acts[rows, :f] = (w * hidden).astype(jnp.bfloat16)
        acts[rows, f:2 * f] = (
            grad_hidden * up_pre * sigmoid * (1.0 + gate_pre * (1.0 - sigmoid))
        ).astype(jnp.bfloat16)
        acts[rows, 2 * f:] = (grad_hidden * silu).astype(jnp.bfloat16)
        act_copy(j).start()
        total = jnp.sum(hidden * grad_scaled, axis=1, keepdims=True)
        wide = jnp.concatenate([jnp.broadcast_to(total, (cap, LANES))] * per_row, axis=0)
        comb[source] = wide.T[:8]
        comb_send(source, mate)
        if j:
            comb_send(source, tp)
        else:
            @pl.when(source == ep)
            def _():
                comb_ret[ep] = comb[ep]

            @pl.when(source != ep)
            def _():
                comb_send(source, tp)

    def slots_back(j, gate):
        act_copy(j).wait_recv()
        rows = block(layers[j], 2 * cap)
        value = dot(acts[rows, f:2 * f], w_gate[...], 1, 1) + dot(acts[rows, 2 * f:], w_up[...], 1, 1)
        slot[rows] = value.astype(jnp.bfloat16)
        for b in range(2):
            target = 2 * layers[j] + lax.rem(column + b, 2)
            if j == b == 0:
                ret[block(ep)] = slot[block(ep)]
            else:
                remote(
                    slot.at[block(target)], ret.at[block(ep)], sem_ret, 1, 0, (target, tp)
                ).start()

    def tables(k, gate):
        relay_table(k)

    def grads(which, gate):
        if which == 0:
            down_grad[...] = dot(acts[:, :f], recv_c[...], 0, 0)
        elif which == 1:
            gate_grad[...] = dot(recv_t[...], acts[:, f:2 * f], 0, 0)
        else:
            up_grad[...] = dot(recv_t[...], acts[:, 2 * f:], 0, 0)

    names = {
        "w": weights_out,
        "T": tables, "rt": relay_tokens, "rc": relay_cots, "pt": parts_tokens, "pc": parts_cots,
        "st": pair_tokens, "sc": pair_cots, "a": act, "b": slots_back, "g": grads,
    }
    outer_order = (
        "pt0", "st0", "pt1", "w0", "pc0", "sc0", "st1", "pc1", "sc1", "a0", "pt3", "w1",
        "b0", "st3", "a1", "pc3", "b1", "sc3", "pt2", "st2", "a3", "pc2", "b3", "sc2",
        "a2", "b2",
    )
    inner_order = (
        "pt0", "w0", "T1", "T0", "st0", "pc0", "rt1", "sc0", "rc1", "a0", "pt3", "w1",
        "rt0", "b0", "st3", "pt1", "rc0", "st1", "pc3", "sc3", "pc1", "pt2", "sc1", "st2",
        "pc2", "a3", "b3", "sc2", "a1", "b1", "a2", "b2",
    )
    for role, order, gate in ((is_outer, outer_order, False), (is_inner, inner_order, True)):
        @pl.when(role)
        def _():
            for word in order:
                with jax.named_scope(word):
                    names[word[:-1]](int(word[-1]), gate)

    for which in range(3):
        with jax.named_scope("g%d" % which):
            grads(which, None)

    with jax.named_scope("cret"):
        own_half = core == column

        @pl.when(own_half)
        def _():
            wait_landed(comb_ret.at[0:peers - 1], sem_cret, 0)

        @pl.when(jnp.logical_not(own_half))
        def _():
            wait_landed(comb_ret, sem_cret, 0)

    part_lane = lax.broadcasted_iota(jnp.int32, (1, LANES), 1)
    totals = [jnp.zeros((1, tokens.shape[0]), jnp.float32)] * 2
    for q in range(slots // LANES):
        row = comb_ret[q * per_row][0:1]
        for r in range(1, per_row):
            row = jnp.where(part_lane >= r * cap, comb_ret[q * per_row + r][0:1], row)
        values = jnp.broadcast_to(row, (LANES, LANES)).T[:, 0:1]
        for k in range(2):
            chosen = onehot_k[k, q * LANES:(q + 1) * LANES] * values
            totals[k] = totals[k] + jnp.sum(chosen, axis=0, keepdims=True)
    for k in range(2):
        grad_combine[k:k + 1] = totals[k]
    with jax.named_scope("ret"):
        wait_landed(ret.at[block(0, (peers - 1) * cap)], sem_ret, 0)
    with jax.named_scope("fin"):
        grad_tokens[...] = dot(gather[...], ret[...], 0, 0).astype(jnp.bfloat16)
    with jax.named_scope("sends"):
        send_e.wait_send()
        wait_sent(send_t.at[block(0, (half - 1) * cap)], sem_t, 2)
        wait_sent(send_c.at[block(0, (half - 1) * cap)], sem_c, 2)
        wait_sent(cross_t, sem_x, 4)
        wait_sent(wrecv.at[0:peers - 1], sem_w, 2)
        wait_sent(core_t, sem_core, 2 * pairs)
        wait_sent(core_c, sem_core, 2 * pairs + 1)
        wait_sent(pair_t, sem_pair, 2 * pairs)
        wait_sent(pair_c, sem_pair, 2 * pairs + 1)
        wait_sent(acts.at[block(0, pairs * cap)], sem_act, pairs)
        wait_sent(slot.at[block(0, (peers - 1) * cap)], sem_ret, 1)

        @pl.when(own_half)
        def _():
            wait_sent(comb.at[0:peers - 1], sem_cret, 1)

        @pl.when(jnp.logical_not(own_half))
        def _():
            wait_sent(comb, sem_cret, 1)

        @pl.when(is_inner)
        def _():
            wait_sent(recv_t.at[block(0, 2 * (half - 1) * cap)], sem_rt, 2)
            wait_sent(recv_t.at[block(0, 2 * (half - 1) * cap)], sem_rc, 2)


def store_kernel(count, *refs):
    sources, targets, sems = refs[:count], refs[count:2 * count], refs[2 * count]
    copies = [
        pltpu.make_async_copy(source, target, sems.at[i])
        for i, (source, target) in enumerate(zip(sources, targets))
    ]
    for copy in copies:
        copy.start()
    for copy in copies:
        copy.wait()


def fused_body(peers, parts, tokens, cotangent, experts, combine, w_gate, w_up, w_down):
    count, width = tokens.shape
    f = w_gate.shape[2]
    picks = experts.shape[1]
    cap = 2 * count * picks // peers
    slots = peers * cap
    pairs = peers // 2
    bf16, f32 = jnp.bfloat16, jnp.float32
    dma = pltpu.SemaphoreType.DMA
    vmem = pl.BlockSpec(memory_space=pltpu.VMEM)
    hbm = pl.BlockSpec(memory_space=pltpu.HBM)
    shapes = (
        jax.ShapeDtypeStruct((count, width), bf16),
        jax.ShapeDtypeStruct((picks, count), f32),
        jax.ShapeDtypeStruct((width, f), f32),
        jax.ShapeDtypeStruct((width, f), f32),
        jax.ShapeDtypeStruct((f, width), f32),
    )
    half_rows = pltpu.VMEM((slots // 2, width), bf16)
    relayed = pltpu.VMEM((2, slots // 2, width), bf16)
    rows = pltpu.VMEM((count, width), bf16)
    crossed = pltpu.VMEM((2, count, width), bf16)
    landed = pltpu.VMEM((slots, width), bf16)
    sums_t = pltpu.VMEM((pairs, cap, 2 * f), bf16)
    sums_c = pltpu.VMEM((pairs, cap, f), bf16)
    small = pltpu.VMEM((peers, 8, LANES), f32)
    outs = pl.pallas_call(
        functools.partial(fused_kernel, peers, parts),
        out_shape=shapes,
        in_specs=[hbm] * 7,
        out_specs=(vmem,) * 5,
        scratch_shapes=[
            rows, rows, pltpu.VMEM((picks, count), jnp.int32), pltpu.VMEM((picks, count), f32),
            pltpu.VMEM((width, f), bf16), pltpu.VMEM((width, f), bf16), pltpu.VMEM((f, width), bf16),
            half_rows, half_rows, crossed, crossed, pltpu.VMEM((2, picks, count), jnp.int32),
            relayed, relayed, landed, landed,
            pltpu.VMEM((slots // LANES, 8, LANES), f32), small,
            pltpu.VMEM((pairs, 2 * cap, 2 * f), bf16), pltpu.VMEM((pairs, 2 * cap, f), bf16),
            sums_t, sums_c, sums_t, sums_c, sums_t, sums_c,
            pltpu.VMEM((slots, 3 * f), bf16), small, landed, landed,
            small, pltpu.VMEM((slots, count), bf16), pltpu.VMEM((2, slots // 2, count), bf16),
            pltpu.VMEM((picks, slots, count), f32),
            dma((7,)), dma((3,)), dma((3,)), dma((3,)), dma((3,)), dma((5,)), dma((3,)), dma((3,)),
            dma((2 * pairs + 2,)), dma((2 * pairs + 2,)), dma((pairs + 1,)), dma((2,)), dma((2,)),
        ],
        compiler_params=pltpu.CompilerParams(
            collective_id=0, has_side_effects=True, vmem_limit_bytes=48 * 1024 * 1024
        ),
    )(*(
        pltpu.with_memory_space_constraint(x, pltpu.HBM)
        for x in (tokens, cotangent, experts.T, combine.T, w_gate, w_up, w_down)
    ))
    outs = pl.pallas_call(
        functools.partial(store_kernel, len(outs)),
        out_shape=shapes,
        in_specs=[vmem] * 5,
        out_specs=(hbm,) * 5,
        scratch_shapes=[dma((5,))],
        compiler_params=pltpu.CompilerParams(vmem_limit_bytes=1024 * 1024),
    )(*outs)
    return outs[0], outs[1].T, outs[2][None], outs[3][None], outs[4][None]


def choose(mesh, tokens, cotangent, experts, combine, w_gate, w_up, w_down):
    peers, parts = mesh.shape["ep"], mesh.shape["tp"]
    count, width = tokens.shape
    cap = 2 * count * experts.shape[1] // w_gate.shape[0] // peers
    fits = (
        w_gate.shape[0] == 1 and experts.shape[1] == 2 and parts == 4
        and peers == 8 and cap in (16, 32, 64, 128)
        and count % LANES == 0 and width % LANES == 0
        and w_gate.shape[2] % LANES == 0 and peers * cap % LANES == 0
    )
    run = functools.partial(fused_body, peers, parts) if fits else body
    return run(tokens, cotangent, experts, combine, w_gate, w_up, w_down)


def solution(mesh):
    return jax.shard_map(
        functools.partial(choose, mesh),
        mesh=mesh,
        in_specs=(
            P("ep", "tp"),
            P("ep", "tp"),
            P("ep", None),
            P("ep", None),
            P("ep", "tp", None),
            P("ep", "tp", None),
            P("ep", None, "tp"),
        ),
        out_specs=(
            P("ep", "tp"),
            P("ep", None),
            P("ep", "tp", None),
            P("ep", "tp", None),
            P("ep", None, "tp"),
        ),
        check_vma=False,
    )
```

```python
import functools

import jax
import jax.numpy as jnp
from jax import lax
from jax.experimental import pallas as pl
from jax.experimental.pallas import tpu as pltpu
from jax.sharding import PartitionSpec as P


def slot_positions(routed, total_experts, capacity):
    onehot = (routed[:, None] == jnp.arange(total_experts, dtype=jnp.int32)[None, :]).astype(
        jnp.int32
    )
    earlier = jnp.sum((jnp.cumsum(onehot, axis=0) - onehot) * onehot, axis=1)
    return routed * capacity + earlier


def activation(gate_pre, up_pre, grad_scaled, weight_grid):
    sigmoid_val = jax.nn.sigmoid(gate_pre)
    silu_val = gate_pre * sigmoid_val
    hidden = silu_val * up_pre
    scaled = (weight_grid * hidden).astype(jnp.bfloat16)
    comb_part = jnp.sum(hidden * grad_scaled, axis=3)
    grad_hidden = weight_grid * grad_scaled
    grad_gate_pre = (
        grad_hidden * up_pre * sigmoid_val * (1.0 + gate_pre * (1.0 - sigmoid_val))
    ).astype(jnp.bfloat16)
    grad_up_pre = (grad_hidden * silu_val).astype(jnp.bfloat16)
    return (scaled, grad_gate_pre, grad_up_pre, comb_part)


def body(tokens, cotangent, experts, combine, w_gate, w_up, w_down):
    peers = lax.axis_size("ep")
    local_experts = w_gate.shape[0]
    total_experts = local_experts * peers
    tok_count = tokens.shape[0]
    picks = experts.shape[1]
    assigns = tok_count * picks
    capacity = 2 * assigns // total_experts
    per_peer = local_experts * capacity
    block_width = tokens.shape[1]
    slot_index = slot_positions(experts.reshape(assigns), total_experts, capacity)
    slot_owner = (
        jnp.zeros((total_experts * capacity,), jnp.int32)
        .at[slot_index]
        .set(jnp.arange(assigns, dtype=jnp.int32) + 1)
    )
    filled = slot_owner > 0
    source = jnp.maximum(slot_owner - 1, 0)
    token_ids = source // picks
    filled_col = filled[:, None]
    send_rows = jnp.where(
        filled_col, jnp.take(tokens, token_ids, axis=0), jnp.zeros((), jnp.bfloat16)
    ).reshape(peers, per_peer, block_width)
    send_cots = jnp.where(
        filled_col, jnp.take(cotangent, token_ids, axis=0), jnp.zeros((), jnp.bfloat16)
    ).reshape(peers, per_peer, block_width)
    send_weights = (
        jnp.where(filled, jnp.take(combine.reshape(assigns), source), jnp.float32(0.0))
        .astype(jnp.bfloat16)
        .reshape(peers, per_peer)
    )
    recv_rows, recv_cots, recv_weights = (
        lax.all_to_all(send_rows, "ep", split_axis=0, concat_axis=0, tiled=True),
        lax.all_to_all(send_cots, "ep", split_axis=0, concat_axis=0, tiled=True),
        lax.all_to_all(send_weights, "ep", split_axis=0, concat_axis=0, tiled=True),
    )
    rows_grid = recv_rows.reshape(peers, local_experts, capacity, block_width)
    cots_grid = recv_cots.reshape(peers, local_experts, capacity, block_width)
    weight_grid = recv_weights.astype(jnp.float32).reshape(peers, local_experts, capacity, 1)
    gate_part = jnp.einsum(
        "secd,edf->secf", rows_grid, w_gate, preferred_element_type=jnp.float32
    ).astype(jnp.bfloat16)
    up_part = jnp.einsum(
        "secd,edf->secf", rows_grid, w_up, preferred_element_type=jnp.float32
    ).astype(jnp.bfloat16)
    down_part = jnp.einsum(
        "secd,efd->secf", cots_grid, w_down, preferred_element_type=jnp.float32
    ).astype(jnp.bfloat16)
    gate_pre, up_pre, grad_scaled = (
        lax.psum(gate_part, "tp").astype(jnp.float32),
        lax.psum(up_part, "tp").astype(jnp.float32),
        lax.psum(down_part, "tp").astype(jnp.float32),
    )
    scaled, grad_gate_pre, grad_up_pre, comb_part = activation(
        gate_pre, up_pre, grad_scaled, weight_grid
    )
    down_grad = jnp.einsum("secf,secd->efd", scaled, cots_grid, preferred_element_type=jnp.float32)
    gate_grad = jnp.einsum(
        "secd,secf->edf", rows_grid, grad_gate_pre, preferred_element_type=jnp.float32
    )
    up_grad = jnp.einsum(
        "secd,secf->edf", rows_grid, grad_up_pre, preferred_element_type=jnp.float32
    )
    slot_sum = jnp.einsum(
        "secf,edf->secd", grad_gate_pre, w_gate, preferred_element_type=jnp.float32
    )
    slot_sum = slot_sum + jnp.einsum(
        "secf,edf->secd", grad_up_pre, w_up, preferred_element_type=jnp.float32
    )
    slot_grad = slot_sum.astype(jnp.bfloat16).reshape(peers, per_peer, block_width)
    returned = lax.all_to_all(slot_grad, "ep", split_axis=0, concat_axis=0, tiled=True)
    comb_back = lax.all_to_all(
        comb_part.reshape(peers, per_peer), "ep", split_axis=0, concat_axis=0, tiled=True
    )
    full_grad = returned.reshape(total_experts * capacity, block_width)
    per_assign = (
        jnp.take(full_grad, slot_index, axis=0)
        .astype(jnp.float32)
        .reshape(tok_count, picks, block_width)
    )
    grad_tokens = jnp.sum(per_assign, axis=1).astype(jnp.bfloat16)
    grad_combine = jnp.take(comb_back.reshape(total_experts * capacity), slot_index).reshape(
        tok_count, picks
    )
    return (grad_tokens, grad_combine, gate_grad, up_grad, down_grad)


MESH = pl.DeviceIdType.MESH
LANES = 128


def flip(index, mask, count):
    result, bit = 0, 1
    while bit < count:
        digit = lax.rem(lax.div(index, bit), 2)
        result = result + bit * ((1 - digit) if mask & bit else digit)
        bit *= 2
    return result


def dot(a, b, ca, cb):
    return lax.dot_general(a, b, (((ca,), (cb,)), ((), ())), preferred_element_type=jnp.float32)


def slot_table(first_expert, second_expert, base, slots, cap):
    count = first_expert.shape[1]
    row = lax.broadcasted_iota(jnp.int32, (slots, count), 0)
    expert = base + lax.shift_right_logical(row, cap.bit_length() - 1)
    number = jnp.bitwise_and(row, cap - 1).astype(jnp.float32)
    first = jnp.where(first_expert == expert, 1.0, 0.0)
    second = jnp.where(second_expert == expert, 1.0, 0.0)
    earlier = jnp.where(
        lax.broadcasted_iota(jnp.int32, (count, count), 0)
        < lax.broadcasted_iota(jnp.int32, (count, count), 1), 1.0, 0.0
    ).astype(jnp.bfloat16)
    position = dot((first + second).astype(jnp.bfloat16), earlier, 1, 0)
    here = jnp.where(position == number, 1.0, 0.0)
    return first * here, second * here


def fused_kernel(
    peers, parts, tokens_hbm, cotangent_hbm, experts_hbm, combine_hbm, gate_hbm, up_hbm, down_hbm,
    ret, gather, grad_combine, gate_grad, up_grad, down_grad,
    tokens, cotangent, experts, combine, w_gate, w_up, w_down,
    send_t, send_c, cross_t, cross_c, cross_e, relay_t, relay_c, recv_t, recv_c,
    wsend, wrecv, part_t, part_c, core_t, core_c, pair_t, pair_c, pair_in_t, pair_in_c,
    acts, comb, slot,
    comb_ret, gather_relay, onehot_k,
    sem_in, sem_t, sem_c, sem_rt, sem_rc, sem_x, sem_w, sem_e,
    sem_core, sem_pair, sem_act, sem_ret, sem_cret,
):
    ep, tp = lax.axis_index("ep"), lax.axis_index("tp")
    core = lax.rem(tp, 2)
    mate = tp + 1 - 2 * core
    across = lax.rem(tp + 2, parts)
    f = w_gate.shape[1]
    slots = recv_t.shape[0]
    cap = slots // peers
    half = peers // 2
    per_row = LANES // cap
    side_of, place = lax.div(ep, half), lax.rem(ep, half)
    peer = [flip(ep, d, peers) for d in range(peers)]
    spot = [lax.rem(p, half) for p in peer]
    layer, column = lax.div(ep, 2), lax.rem(ep, 2)
    inner = jnp.where(layer == 1 + side_of, 1, 0)
    is_inner, is_outer = inner == 1, inner == 0
    layers = (layer, layer + 1 - 2 * lax.rem(layer, 2), 2 - side_of, 3 * (1 - side_of))
    far_gate = (2 * layers[2] + column, tp)

    def block(index, size=cap):
        return pl.ds(pl.multiple_of(index * size, size), size)

    def remote(src, dst, sems, sent, landed, device):
        return pltpu.make_async_remote_copy(
            src_ref=src, dst_ref=dst, send_sem=sems.at[sent], recv_sem=sems.at[landed],
            device_id=device, device_id_type=MESH,
        )

    def wait_sent(ref, sems, sent):
        remote(ref, ref, sems, sent, sent, (ep, mate)).wait_send()

    def wait_landed(ref, sems, landed):
        remote(ref, ref, sems, landed, landed, (ep, mate)).wait_recv()

    loads = [
        pltpu.make_async_copy(source, target, sem_in.at[i])
        for i, (source, target) in enumerate((
            (experts_hbm, experts), (combine_hbm, combine), (tokens_hbm, tokens),
            (cotangent_hbm, cotangent), (gate_hbm.at[0], w_gate), (up_hbm.at[0], w_up),
            (down_hbm.at[0], w_down),
        ))
    ]
    barrier = pltpu.get_barrier_semaphore()
    for device in [(peer[d], tp) for d in range(1, half)] + [(ep, mate), (ep, across)]:
        pl.semaphore_signal(barrier, inc=1, device_id=device, device_id_type=MESH)

    @pl.when(is_inner)
    def _():
        for far in (2, 3):
            device = (2 * layers[far] + column, tp)
            pl.semaphore_signal(barrier, inc=1, device_id=device, device_id_type=MESH)

    for load in loads:
        load.start()
    loads[0].wait()
    loads[1].wait()

    first, second = slot_table(experts[0:1], experts[1:2], 0, slots, cap)
    onehot_k[0] = first
    onehot_k[1] = second
    gather[...] = (first + second).astype(jnp.bfloat16)
    weight = combine[...].astype(jnp.bfloat16).astype(jnp.float32)
    weight_column = jnp.sum(first * weight[0:1] + second * weight[1:2], axis=1, keepdims=True)
    for q in range(slots // LANES):
        wide = jnp.broadcast_to(weight_column[q * LANES:(q + 1) * LANES], (LANES, LANES))
        wsend[q] = wide.T[:8]
    wrecv[ep] = wsend[lax.div(ep, per_row)]
    loads[2].wait()
    loads[3].wait()
    own = gather[block(side_of, half * cap)]
    send_t[...] = dot(own, tokens[...], 1, 0).astype(jnp.bfloat16)
    send_c[...] = dot(own, cotangent[...], 1, 0).astype(jnp.bfloat16)
    with jax.named_scope("barrier"):
        pl.semaphore_wait(barrier, half + 2)

    send_e = remote(experts, cross_e.at[1 - inner], sem_e, 2, 1 - inner, far_gate)
    send_e.start()

    def send_weights(target, far):
        remote(
            wsend.at[lax.div(target, per_row)], wrecv.at[ep], sem_w, 2, far, (target, tp)
        ).start()

    for d in range(1, half):
        send_weights(peer[d], 0)
    remote(tokens, cross_t.at[1 - inner], sem_x, 4, 1 - inner, far_gate).start()
    remote(cotangent, cross_c.at[1 - inner], sem_x, 4, 3 - inner, far_gate).start()

    def near_send(k, d):
        packed, landed, sems = ((send_t, recv_t, sem_t), (send_c, recv_c, sem_c))[k]
        remote(
            packed.at[block(spot[d])], landed.at[block(ep)], sems, 2, min(d - 1, 1), (peer[d], tp)
        ).start()

    near_send(0, 1)
    near_send(1, 1)
    recv_t[block(ep)] = send_t[block(place)]
    recv_c[block(ep)] = send_c[block(place)]

    for load in loads[4:]:
        load.wait()

    def relay_table(k):
        wait_landed(cross_e.at[k], sem_e, k)
        chosen_a, chosen_b = slot_table(
            cross_e[k, 0:1], cross_e[k, 1:2], side_of * half, half * cap, cap
        )
        gather_relay[k] = (chosen_a + chosen_b).astype(jnp.bfloat16)

    def relay(k, landed_in, crossed, packed, landed, sems):
        wait_landed(crossed.at[k], sem_x, landed_in)
        packed[k] = dot(gather_relay[k], crossed[k], 1, 0).astype(jnp.bfloat16)
        rows = block(2 * layers[2 + k] + column)
        for d in (1, 2, 3) if k else (1, 3, 2):
            remote(packed.at[k, block(spot[d])], landed.at[rows], sems, 2, k, (peer[d], tp)).start()
        landed[rows] = packed[k, block(place)]

    def relay_tokens(k, gate):
        relay(k, k, cross_t, relay_t, recv_t, sem_rt)

    def relay_cots(k, gate):
        relay(k, 2 + k, cross_c, relay_c, recv_c, sem_rc)

    def arrive(j, gate, landed, near_sems, sems):
        count = cap if j == 0 or (gate and j > 1) else 2 * cap
        wait_landed(landed.at[block(0, count)], sems if j > 1 else near_sems, j % 2)

    def weights_out(k, gate):
        for b in range(2):
            target = 2 * layers[2 + k] + b
            send_weights(target, 1)

    pairs = peers // 2

    def core_copy(i):
        part, landed = (part_t, core_t) if i < pairs else (part_c, core_c)
        j = i % pairs
        return remote(
            part.at[j, block(1 - core)], landed.at[j], sem_core, 2 * pairs + i // pairs, i, (ep, mate)
        )

    def pair_copy(i):
        summed, landed = (pair_t, pair_in_t) if i < pairs else (pair_c, pair_in_c)
        return remote(
            summed.at[i % pairs], landed.at[i % pairs], sem_pair, 2 * pairs + i // pairs, i,
            (ep, across),
        )

    def act_copy(j):
        rows = block(2 * layers[j] + core)
        return remote(acts.at[rows], acts.at[rows], sem_act, pairs, j, (ep, mate))

    def comb_send(source, device):
        remote(comb.at[source], comb_ret.at[ep], sem_cret, 1, 0, (source, device)).start()

    def parts_tokens(j, gate):
        arrive(j, gate, recv_t, sem_t, sem_rt)
        rows = recv_t[block(layers[j], 2 * cap)]
        part_t[j, :, :f] = dot(rows, w_gate[...], 1, 0).astype(jnp.bfloat16)
        part_t[j, :, f:] = dot(rows, w_up[...], 1, 0).astype(jnp.bfloat16)
        core_copy(j).start()

    def parts_cots(j, gate):
        arrive(j, gate, recv_c, sem_c, sem_rc)
        cots = recv_c[block(layers[j], 2 * cap)]
        part_c[j] = dot(cots, w_down[...], 1, 1).astype(jnp.bfloat16)
        core_copy(pairs + j).start()

    def pair_sum(j, i, part, landed, summed):
        core_copy(i).wait_recv()
        mine = part[j, block(core)].astype(jnp.float32)
        summed[j] = (mine + landed[j].astype(jnp.float32)).astype(jnp.bfloat16)
        pair_copy(i).start()

    def pair_tokens(j, gate):
        pair_sum(j, j, part_t, core_t, pair_t)

    def pair_cots(j, gate):
        pair_sum(j, pairs + j, part_c, core_c, pair_c)

    def act(j, gate):
        if j == 0:
            wait_landed(wrecv.at[0:half - 1], sem_w, 0)
        if j == 3:
            wait_landed(wrecv.at[0:half], sem_w, 1)
        pair_copy(j).wait_recv()
        pair_copy(pairs + j).wait_recv()
        source = 2 * layers[j] + core
        gate_pre = pair_t[j, :, :f].astype(jnp.float32) + pair_in_t[j, :, :f].astype(jnp.float32)
        up_pre = pair_t[j, :, f:].astype(jnp.float32) + pair_in_t[j, :, f:].astype(jnp.float32)
        grad_scaled = pair_c[j].astype(jnp.float32) + pair_in_c[j].astype(jnp.float32)
        weights = jnp.broadcast_to(wrecv[source][0:1], (LANES, LANES)).T
        w = weights[:cap]
        for r in range(1, per_row):
            w = jnp.where(lax.rem(ep, per_row) == r, weights[r * cap:(r + 1) * cap], w)
        w = w[:, 0:1]
        sigmoid = jax.nn.sigmoid(gate_pre)
        silu = gate_pre * sigmoid
        hidden = silu * up_pre
        grad_hidden = w * grad_scaled
        rows = block(source)
        acts[rows, :f] = (w * hidden).astype(jnp.bfloat16)
        acts[rows, f:2 * f] = (
            grad_hidden * up_pre * sigmoid * (1.0 + gate_pre * (1.0 - sigmoid))
        ).astype(jnp.bfloat16)
        acts[rows, 2 * f:] = (grad_hidden * silu).astype(jnp.bfloat16)
        act_copy(j).start()
        total = jnp.sum(hidden * grad_scaled, axis=1, keepdims=True)
        wide = jnp.concatenate([jnp.broadcast_to(total, (cap, LANES))] * per_row, axis=0)
        comb[source] = wide.T[:8]
        comb_send(source, mate)
        if j:
            comb_send(source, tp)
        else:
            @pl.when(source == ep)
            def _():
                comb_ret[ep] = comb[ep]

            @pl.when(source != ep)
            def _():
                comb_send(source, tp)

    def slot_rows(j, half_of):
        source = 2 * layers[j] + half_of
        rows = block(source)
        value = dot(acts[rows, f:2 * f], w_gate[...], 1, 1) + dot(acts[rows, 2 * f:], w_up[...], 1, 1)
        slot[rows] = value.astype(jnp.bfloat16)

        def send():
            remote(slot.at[rows], ret.at[block(ep)], sem_ret, 1, 0, (source, tp)).start()

        if j:
            send()
        else:
            pl.when(source != ep)(send)

            @pl.when(source == ep)
            def _():
                ret[block(ep)] = slot[rows]

    def slots_own(j, gate):
        slot_rows(j, core)

    def slots_mate(j, gate):
        act_copy(j).wait_recv()
        slot_rows(j, 1 - core)

    def tables(k, gate):
        relay_table(k)

    def grads(which, gate):
        if which == 0:
            down_grad[...] = dot(acts[:, :f], recv_c[...], 0, 0)
        elif which == 1:
            gate_grad[...] = dot(recv_t[...], acts[:, f:2 * f], 0, 0)
        else:
            up_grad[...] = dot(recv_t[...], acts[:, 2 * f:], 0, 0)

    def near_sends(k, gate):
        for d in range(half - 1, 1, -1):
            near_send(k, d)

    names = {
        "n": near_sends,
        "w": weights_out,
        "T": tables, "rt": relay_tokens, "rc": relay_cots, "pt": parts_tokens, "pc": parts_cots,
        "st": pair_tokens, "sc": pair_cots, "a": act, "o": slots_own, "b": slots_mate,
        "g": grads,
    }
    outer_order = (
        "n0", "n1", "pt0", "st0", "pt1", "w0", "pc0", "sc0", "st1", "pc1", "sc1", "a0",
        "o0", "pt3", "w1", "st3", "b0", "pc3", "a1", "o1", "sc3", "b1", "pt2", "st2",
        "a3", "o3", "pc2", "b3", "sc2", "a2", "o2", "b2",
    )
    inner_order = (
        "n0", "n1", "pt0", "w0", "T1", "T0", "st0", "pc0", "rt1", "sc0", "rc1", "a0",
        "o0", "pt3", "w1", "st3", "rt0", "b0", "rc0", "pc3", "sc3", "pt1", "st1", "pt2",
        "st2", "pc1", "a3", "o3", "sc1", "pc2", "b3", "sc2", "a1", "o1", "a2", "o2",
        "b1", "b2",
    )
    for role, order, gate in ((is_outer, outer_order, False), (is_inner, inner_order, True)):
        @pl.when(role)
        def _():
            for word in order:
                with jax.named_scope(word):
                    names[word[:-1]](int(word[-1]), gate)

    for which in range(3):
        with jax.named_scope("g%d" % which):
            grads(which, None)

    with jax.named_scope("cret"):
        own_half = core == column

        @pl.when(own_half)
        def _():
            wait_landed(comb_ret.at[0:peers - 1], sem_cret, 0)

        @pl.when(jnp.logical_not(own_half))
        def _():
            wait_landed(comb_ret, sem_cret, 0)

    part_lane = lax.broadcasted_iota(jnp.int32, (1, LANES), 1)
    totals = [jnp.zeros((1, tokens.shape[0]), jnp.float32)] * 2
    for q in range(slots // LANES):
        row = comb_ret[q * per_row][0:1]
        for r in range(1, per_row):
            row = jnp.where(part_lane >= r * cap, comb_ret[q * per_row + r][0:1], row)
        values = jnp.broadcast_to(row, (LANES, LANES)).T[:, 0:1]
        for k in range(2):
            chosen = onehot_k[k, q * LANES:(q + 1) * LANES] * values
            totals[k] = totals[k] + jnp.sum(chosen, axis=0, keepdims=True)
    for k in range(2):
        grad_combine[k:k + 1] = totals[k]
    with jax.named_scope("ret"):
        wait_landed(ret.at[block(0, (peers - 1) * cap)], sem_ret, 0)
    with jax.named_scope("sends"):
        send_e.wait_send()
        wait_sent(send_t.at[block(0, (half - 1) * cap)], sem_t, 2)
        wait_sent(send_c.at[block(0, (half - 1) * cap)], sem_c, 2)
        wait_sent(cross_t, sem_x, 4)
        wait_sent(wrecv.at[0:peers - 1], sem_w, 2)
        wait_sent(core_t, sem_core, 2 * pairs)
        wait_sent(core_c, sem_core, 2 * pairs + 1)
        wait_sent(pair_t, sem_pair, 2 * pairs)
        wait_sent(pair_c, sem_pair, 2 * pairs + 1)
        wait_sent(acts.at[block(0, pairs * cap)], sem_act, pairs)
        wait_sent(slot.at[block(0, (peers - 1) * cap)], sem_ret, 1)

        @pl.when(own_half)
        def _():
            wait_sent(comb.at[0:peers - 1], sem_cret, 1)

        @pl.when(jnp.logical_not(own_half))
        def _():
            wait_sent(comb, sem_cret, 1)

        @pl.when(is_inner)
        def _():
            wait_sent(recv_t.at[block(0, 2 * (half - 1) * cap)], sem_rt, 2)
            wait_sent(recv_t.at[block(0, 2 * (half - 1) * cap)], sem_rc, 2)


def store_kernel(ret, gather, *refs):
    count = (len(refs) - 2) // 2
    sources, first, targets = refs[:count], refs[count], refs[count + 1:2 * count + 1]
    grad_tokens, sems = refs[-2:]
    copies = [
        pltpu.make_async_copy(source, target, sems.at[i])
        for i, (source, target) in enumerate(zip((*sources, grad_tokens), (*targets, first)))
    ]
    for copy in copies[:count]:
        copy.start()
    grad_tokens[...] = dot(gather[...], ret[...], 0, 0).astype(jnp.bfloat16)
    copies[count].start()
    for copy in copies:
        copy.wait()


def fused_body(peers, parts, tokens, cotangent, experts, combine, w_gate, w_up, w_down):
    count, width = tokens.shape
    f = w_gate.shape[2]
    picks = experts.shape[1]
    cap = 2 * count * picks // peers
    slots = peers * cap
    pairs = peers // 2
    bf16, f32 = jnp.bfloat16, jnp.float32
    dma = pltpu.SemaphoreType.DMA
    vmem = pl.BlockSpec(memory_space=pltpu.VMEM)
    hbm = pl.BlockSpec(memory_space=pltpu.HBM)
    shapes = (
        jax.ShapeDtypeStruct((count, width), bf16),
        jax.ShapeDtypeStruct((picks, count), f32),
        jax.ShapeDtypeStruct((width, f), f32),
        jax.ShapeDtypeStruct((width, f), f32),
        jax.ShapeDtypeStruct((f, width), f32),
    )
    half_rows = pltpu.VMEM((slots // 2, width), bf16)
    relayed = pltpu.VMEM((2, slots // 2, width), bf16)
    rows = pltpu.VMEM((count, width), bf16)
    crossed = pltpu.VMEM((2, count, width), bf16)
    landed = pltpu.VMEM((slots, width), bf16)
    sums_t = pltpu.VMEM((pairs, cap, 2 * f), bf16)
    sums_c = pltpu.VMEM((pairs, cap, f), bf16)
    small = pltpu.VMEM((peers, 8, LANES), f32)
    outs = pl.pallas_call(
        functools.partial(fused_kernel, peers, parts),
        out_shape=(
            jax.ShapeDtypeStruct((slots, width), bf16), jax.ShapeDtypeStruct((slots, count), bf16),
            *shapes[1:],
        ),
        in_specs=[hbm] * 7,
        out_specs=(vmem,) * 6,
        scratch_shapes=[
            rows, rows, pltpu.VMEM((picks, count), jnp.int32), pltpu.VMEM((picks, count), f32),
            pltpu.VMEM((width, f), bf16), pltpu.VMEM((width, f), bf16), pltpu.VMEM((f, width), bf16),
            half_rows, half_rows, crossed, crossed, pltpu.VMEM((2, picks, count), jnp.int32),
            relayed, relayed, landed, landed,
            pltpu.VMEM((slots // LANES, 8, LANES), f32), small,
            pltpu.VMEM((pairs, 2 * cap, 2 * f), bf16), pltpu.VMEM((pairs, 2 * cap, f), bf16),
            sums_t, sums_c, sums_t, sums_c, sums_t, sums_c,
            pltpu.VMEM((slots, 3 * f), bf16), small, landed,
            small, pltpu.VMEM((2, slots // 2, count), bf16),
            pltpu.VMEM((picks, slots, count), f32),
            dma((7,)), dma((3,)), dma((3,)), dma((3,)), dma((3,)), dma((5,)), dma((3,)), dma((3,)),
            dma((2 * pairs + 2,)), dma((2 * pairs + 2,)), dma((pairs + 1,)), dma((2,)), dma((2,)),
        ],
        compiler_params=pltpu.CompilerParams(
            collective_id=0, has_side_effects=True, vmem_limit_bytes=48 * 1024 * 1024
        ),
    )(*(
        pltpu.with_memory_space_constraint(x, pltpu.HBM)
        for x in (tokens, cotangent, experts.T, combine.T, w_gate, w_up, w_down)
    ))
    outs = pl.pallas_call(
        store_kernel,
        out_shape=shapes,
        in_specs=[vmem] * 6,
        out_specs=(hbm,) * 5,
        scratch_shapes=[rows, dma((5,))],
        compiler_params=pltpu.CompilerParams(vmem_limit_bytes=4 * 1024 * 1024),
    )(*outs)
    return outs[0], outs[1].T, outs[2][None], outs[3][None], outs[4][None]


def choose(mesh, tokens, cotangent, experts, combine, w_gate, w_up, w_down):
    peers, parts = mesh.shape["ep"], mesh.shape["tp"]
    count, width = tokens.shape
    cap = 2 * count * experts.shape[1] // w_gate.shape[0] // peers
    fits = (
        w_gate.shape[0] == 1 and experts.shape[1] == 2 and parts == 4
        and peers == 8 and cap in (16, 32, 64, 128)
        and count % LANES == 0 and width % LANES == 0
        and w_gate.shape[2] % LANES == 0 and peers * cap % LANES == 0
    )
    run = functools.partial(fused_body, peers, parts) if fits else body
    return run(tokens, cotangent, experts, combine, w_gate, w_up, w_down)


def solution(mesh):
    return jax.shard_map(
        functools.partial(choose, mesh),
        mesh=mesh,
        in_specs=(
            P("ep", "tp"),
            P("ep", "tp"),
            P("ep", None),
            P("ep", None),
            P("ep", "tp", None),
            P("ep", "tp", None),
            P("ep", None, "tp"),
        ),
        out_specs=(
            P("ep", "tp"),
            P("ep", None),
            P("ep", "tp", None),
            P("ep", "tp", None),
            P("ep", None, "tp"),
        ),
        check_vma=False,
    )
```

```python
import functools

import jax
import jax.numpy as jnp
from jax import lax
from jax.experimental import pallas as pl
from jax.experimental.pallas import tpu as pltpu
from jax.sharding import PartitionSpec as P


def slot_positions(routed, total_experts, capacity):
    onehot = (routed[:, None] == jnp.arange(total_experts, dtype=jnp.int32)[None, :]).astype(
        jnp.int32
    )
    earlier = jnp.sum((jnp.cumsum(onehot, axis=0) - onehot) * onehot, axis=1)
    return routed * capacity + earlier


def activation(gate_pre, up_pre, grad_scaled, weight_grid):
    sigmoid_val = jax.nn.sigmoid(gate_pre)
    silu_val = gate_pre * sigmoid_val
    hidden = silu_val * up_pre
    scaled = (weight_grid * hidden).astype(jnp.bfloat16)
    comb_part = jnp.sum(hidden * grad_scaled, axis=3)
    grad_hidden = weight_grid * grad_scaled
    grad_gate_pre = (
        grad_hidden * up_pre * sigmoid_val * (1.0 + gate_pre * (1.0 - sigmoid_val))
    ).astype(jnp.bfloat16)
    grad_up_pre = (grad_hidden * silu_val).astype(jnp.bfloat16)
    return (scaled, grad_gate_pre, grad_up_pre, comb_part)


def body(tokens, cotangent, experts, combine, w_gate, w_up, w_down):
    peers = lax.axis_size("ep")
    local_experts = w_gate.shape[0]
    total_experts = local_experts * peers
    tok_count = tokens.shape[0]
    picks = experts.shape[1]
    assigns = tok_count * picks
    capacity = 2 * assigns // total_experts
    per_peer = local_experts * capacity
    block_width = tokens.shape[1]
    slot_index = slot_positions(experts.reshape(assigns), total_experts, capacity)
    slot_owner = (
        jnp.zeros((total_experts * capacity,), jnp.int32)
        .at[slot_index]
        .set(jnp.arange(assigns, dtype=jnp.int32) + 1)
    )
    filled = slot_owner > 0
    source = jnp.maximum(slot_owner - 1, 0)
    token_ids = source // picks
    filled_col = filled[:, None]
    send_rows = jnp.where(
        filled_col, jnp.take(tokens, token_ids, axis=0), jnp.zeros((), jnp.bfloat16)
    ).reshape(peers, per_peer, block_width)
    send_cots = jnp.where(
        filled_col, jnp.take(cotangent, token_ids, axis=0), jnp.zeros((), jnp.bfloat16)
    ).reshape(peers, per_peer, block_width)
    send_weights = (
        jnp.where(filled, jnp.take(combine.reshape(assigns), source), jnp.float32(0.0))
        .astype(jnp.bfloat16)
        .reshape(peers, per_peer)
    )
    recv_rows, recv_cots, recv_weights = (
        lax.all_to_all(send_rows, "ep", split_axis=0, concat_axis=0, tiled=True),
        lax.all_to_all(send_cots, "ep", split_axis=0, concat_axis=0, tiled=True),
        lax.all_to_all(send_weights, "ep", split_axis=0, concat_axis=0, tiled=True),
    )
    rows_grid = recv_rows.reshape(peers, local_experts, capacity, block_width)
    cots_grid = recv_cots.reshape(peers, local_experts, capacity, block_width)
    weight_grid = recv_weights.astype(jnp.float32).reshape(peers, local_experts, capacity, 1)
    gate_part = jnp.einsum(
        "secd,edf->secf", rows_grid, w_gate, preferred_element_type=jnp.float32
    ).astype(jnp.bfloat16)
    up_part = jnp.einsum(
        "secd,edf->secf", rows_grid, w_up, preferred_element_type=jnp.float32
    ).astype(jnp.bfloat16)
    down_part = jnp.einsum(
        "secd,efd->secf", cots_grid, w_down, preferred_element_type=jnp.float32
    ).astype(jnp.bfloat16)
    gate_pre, up_pre, grad_scaled = (
        lax.psum(gate_part, "tp").astype(jnp.float32),
        lax.psum(up_part, "tp").astype(jnp.float32),
        lax.psum(down_part, "tp").astype(jnp.float32),
    )
    scaled, grad_gate_pre, grad_up_pre, comb_part = activation(
        gate_pre, up_pre, grad_scaled, weight_grid
    )
    down_grad = jnp.einsum("secf,secd->efd", scaled, cots_grid, preferred_element_type=jnp.float32)
    gate_grad = jnp.einsum(
        "secd,secf->edf", rows_grid, grad_gate_pre, preferred_element_type=jnp.float32
    )
    up_grad = jnp.einsum(
        "secd,secf->edf", rows_grid, grad_up_pre, preferred_element_type=jnp.float32
    )
    slot_sum = jnp.einsum(
        "secf,edf->secd", grad_gate_pre, w_gate, preferred_element_type=jnp.float32
    )
    slot_sum = slot_sum + jnp.einsum(
        "secf,edf->secd", grad_up_pre, w_up, preferred_element_type=jnp.float32
    )
    slot_grad = slot_sum.astype(jnp.bfloat16).reshape(peers, per_peer, block_width)
    returned = lax.all_to_all(slot_grad, "ep", split_axis=0, concat_axis=0, tiled=True)
    comb_back = lax.all_to_all(
        comb_part.reshape(peers, per_peer), "ep", split_axis=0, concat_axis=0, tiled=True
    )
    full_grad = returned.reshape(total_experts * capacity, block_width)
    per_assign = (
        jnp.take(full_grad, slot_index, axis=0)
        .astype(jnp.float32)
        .reshape(tok_count, picks, block_width)
    )
    grad_tokens = jnp.sum(per_assign, axis=1).astype(jnp.bfloat16)
    grad_combine = jnp.take(comb_back.reshape(total_experts * capacity), slot_index).reshape(
        tok_count, picks
    )
    return (grad_tokens, grad_combine, gate_grad, up_grad, down_grad)


MESH = pl.DeviceIdType.MESH
LANES = 128


def flip(index, mask, count):
    result, bit = 0, 1
    while bit < count:
        digit = lax.rem(lax.div(index, bit), 2)
        result = result + bit * ((1 - digit) if mask & bit else digit)
        bit *= 2
    return result


def dot(a, b, ca, cb):
    return lax.dot_general(a, b, (((ca,), (cb,)), ((), ())), preferred_element_type=jnp.float32)


def slot_table(first_expert, second_expert, base, slots, cap):
    count = first_expert.shape[1]
    row = lax.broadcasted_iota(jnp.int32, (slots, count), 0)
    expert = base + lax.shift_right_logical(row, cap.bit_length() - 1)
    number = jnp.bitwise_and(row, cap - 1).astype(jnp.float32)
    first = jnp.where(first_expert == expert, 1.0, 0.0)
    second = jnp.where(second_expert == expert, 1.0, 0.0)
    earlier = jnp.where(
        lax.broadcasted_iota(jnp.int32, (count, count), 0)
        < lax.broadcasted_iota(jnp.int32, (count, count), 1), 1.0, 0.0
    ).astype(jnp.bfloat16)
    position = dot((first + second).astype(jnp.bfloat16), earlier, 1, 0)
    here = jnp.where(position == number, 1.0, 0.0)
    return first * here, second * here


def fused_kernel(
    peers, parts, tokens_hbm, cotangent_hbm, experts_hbm, combine_hbm, gate_hbm, up_hbm, down_hbm,
    ret, gather, grad_combine, gate_grad, up_grad, down_grad,
    tokens, cotangent, experts, combine, w_gate, w_up, w_down, w_slot, w_part,
    send_t, send_c, cross_t, cross_c, cross_e, relay_t, relay_c, recv_t, recv_c,
    wsend, wrecv, part_t, part_c, core_t, core_c, pair_t, pair_c, pair_in_t, pair_in_c,
    acts, comb, slot,
    comb_ret, gather_relay, onehot_k,
    sem_in, sem_t, sem_c, sem_rt, sem_rc, sem_x, sem_w, sem_e,
    sem_core, sem_pair, sem_act, sem_ret, sem_cret,
):
    ep, tp = lax.axis_index("ep"), lax.axis_index("tp")
    core = lax.rem(tp, 2)
    mate = tp + 1 - 2 * core
    across = lax.rem(tp + 2, parts)
    f = w_gate.shape[1]
    slots = recv_t.shape[0]
    cap = slots // peers
    half = peers // 2
    per_row = LANES // cap
    side_of, place = lax.div(ep, half), lax.rem(ep, half)
    peer = [flip(ep, d, peers) for d in range(peers)]
    spot = [lax.rem(p, half) for p in peer]
    layer, column = lax.div(ep, 2), lax.rem(ep, 2)
    inner = jnp.where(layer == 1 + side_of, 1, 0)
    is_inner, is_outer = inner == 1, inner == 0
    layers = (layer, layer + 1 - 2 * lax.rem(layer, 2), 2 - side_of, 3 * (1 - side_of))
    far_gate = (2 * layers[2] + column, tp)

    def block(index, size=cap):
        return pl.ds(pl.multiple_of(index * size, size), size)

    def remote(src, dst, sems, sent, landed, device):
        return pltpu.make_async_remote_copy(
            src_ref=src, dst_ref=dst, send_sem=sems.at[sent], recv_sem=sems.at[landed],
            device_id=device, device_id_type=MESH,
        )

    def wait_sent(ref, sems, sent):
        remote(ref, ref, sems, sent, sent, (ep, mate)).wait_send()

    def wait_landed(ref, sems, landed):
        remote(ref, ref, sems, landed, landed, (ep, mate)).wait_recv()

    loads = [
        pltpu.make_async_copy(source, target, sem_in.at[i])
        for i, (source, target) in enumerate((
            (experts_hbm, experts), (combine_hbm, combine), (tokens_hbm, tokens),
            (cotangent_hbm, cotangent), (gate_hbm.at[0], w_gate), (up_hbm.at[0], w_up),
            (down_hbm.at[0], w_down),
        ))
    ]
    barrier = pltpu.get_barrier_semaphore()
    for device in [(peer[d], tp) for d in range(1, half)] + [(ep, mate), (ep, across)]:
        pl.semaphore_signal(barrier, inc=1, device_id=device, device_id_type=MESH)

    @pl.when(is_inner)
    def _():
        for far in (2, 3):
            device = (2 * layers[far] + column, tp)
            pl.semaphore_signal(barrier, inc=1, device_id=device, device_id_type=MESH)

    for load in loads:
        load.start()
    loads[0].wait()
    loads[1].wait()

    first, second = slot_table(experts[0:1], experts[1:2], 0, slots, cap)
    onehot_k[0] = first
    onehot_k[1] = second
    gather[...] = (first + second).astype(jnp.bfloat16)
    weight = combine[...].astype(jnp.bfloat16).astype(jnp.float32)
    weight_column = jnp.sum(first * weight[0:1] + second * weight[1:2], axis=1, keepdims=True)
    for q in range(slots // LANES):
        wide = jnp.broadcast_to(weight_column[q * LANES:(q + 1) * LANES], (LANES, LANES))
        wsend[q] = wide.T[:8]
    wrecv[ep] = wsend[lax.div(ep, per_row)]
    loads[2].wait()
    loads[3].wait()
    own = gather[block(side_of, half * cap)]
    send_t[...] = dot(own, tokens[...], 1, 0).astype(jnp.bfloat16)
    send_c[...] = dot(own, cotangent[...], 1, 0).astype(jnp.bfloat16)
    with jax.named_scope("barrier"):
        pl.semaphore_wait(barrier, half + 2)

    send_e = remote(experts, cross_e.at[1 - inner], sem_e, 2, 1 - inner, far_gate)
    send_e.start()

    def send_weights(target, far):
        remote(
            wsend.at[lax.div(target, per_row)], wrecv.at[ep], sem_w, 2, far, (target, tp)
        ).start()

    for d in range(1, half):
        send_weights(peer[d], 0)
    remote(tokens, cross_t.at[1 - inner], sem_x, 4, 1 - inner, far_gate).start()
    remote(cotangent, cross_c.at[1 - inner], sem_x, 4, 3 - inner, far_gate).start()

    def near_send(k, d):
        packed, landed, sems = ((send_t, recv_t, sem_t), (send_c, recv_c, sem_c))[k]
        remote(
            packed.at[block(spot[d])], landed.at[block(ep)], sems, 2, min(d - 1, 1), (peer[d], tp)
        ).start()

    near_send(0, 1)
    near_send(1, 1)
    recv_t[block(ep)] = send_t[block(place)]
    recv_c[block(ep)] = send_c[block(place)]

    for load in loads[4:]:
        load.wait()
    with jax.named_scope("transposes"):
        w_slot[:f] = w_gate[...].T
        w_slot[f:] = w_up[...].T
        w_part[...] = w_down[...].T

    def relay_table(k):
        wait_landed(cross_e.at[k], sem_e, k)
        chosen_a, chosen_b = slot_table(
            cross_e[k, 0:1], cross_e[k, 1:2], side_of * half, half * cap, cap
        )
        gather_relay[k] = (chosen_a + chosen_b).astype(jnp.bfloat16)

    def relay(k, landed_in, crossed, packed, landed, sems):
        wait_landed(crossed.at[k], sem_x, landed_in)
        packed[k] = dot(gather_relay[k], crossed[k], 1, 0).astype(jnp.bfloat16)
        rows = block(2 * layers[2 + k] + column)
        for d in (1, 2, 3) if k else (1, 3, 2):
            remote(packed.at[k, block(spot[d])], landed.at[rows], sems, 2, k, (peer[d], tp)).start()
        landed[rows] = packed[k, block(place)]

    def relay_tokens(k, gate):
        relay(k, k, cross_t, relay_t, recv_t, sem_rt)

    def relay_cots(k, gate):
        relay(k, 2 + k, cross_c, relay_c, recv_c, sem_rc)

    def arrive(j, gate, landed, near_sems, sems):
        count = cap if j == 0 or (gate and j > 1) else 2 * cap
        wait_landed(landed.at[block(0, count)], sems if j > 1 else near_sems, j % 2)

    def weights_out(k, gate):
        for b in range(2):
            target = 2 * layers[2 + k] + b
            send_weights(target, 1)

    pairs = peers // 2

    def core_copy(i):
        part, landed = (part_t, core_t) if i < pairs else (part_c, core_c)
        j = i % pairs
        return remote(
            part.at[j, block(1 - core)], landed.at[j], sem_core, 2 * pairs + i // pairs, i, (ep, mate)
        )

    def pair_copy(i):
        summed, landed = (pair_t, pair_in_t) if i < pairs else (pair_c, pair_in_c)
        return remote(
            summed.at[i % pairs], landed.at[i % pairs], sem_pair, 2 * pairs + i // pairs, i,
            (ep, across),
        )

    def act_copy(j):
        rows = block(2 * layers[j] + core)
        return remote(acts.at[rows], acts.at[rows], sem_act, pairs, j, (ep, mate))

    def comb_send(source, device):
        remote(comb.at[source], comb_ret.at[ep], sem_cret, 1, 0, (source, device)).start()

    def parts_tokens(j, gate):
        arrive(j, gate, recv_t, sem_t, sem_rt)
        rows = recv_t[block(layers[j], 2 * cap)]
        part_t[j, :, :f] = dot(rows, w_gate[...], 1, 0).astype(jnp.bfloat16)
        part_t[j, :, f:] = dot(rows, w_up[...], 1, 0).astype(jnp.bfloat16)
        core_copy(j).start()

    def parts_cots(j, gate):
        arrive(j, gate, recv_c, sem_c, sem_rc)
        cots = recv_c[block(layers[j], 2 * cap)]
        part_c[j] = dot(cots, w_part[...], 1, 0).astype(jnp.bfloat16)
        core_copy(pairs + j).start()

    def pair_sum(j, i, part, landed, summed):
        core_copy(i).wait_recv()
        mine = part[j, block(core)].astype(jnp.float32)
        summed[j] = (mine + landed[j].astype(jnp.float32)).astype(jnp.bfloat16)
        pair_copy(i).start()

    def pair_tokens(j, gate):
        pair_sum(j, j, part_t, core_t, pair_t)

    def pair_cots(j, gate):
        pair_sum(j, pairs + j, part_c, core_c, pair_c)

    def act(j, gate):
        if j == 0:
            wait_landed(wrecv.at[0:half - 1], sem_w, 0)
        if j == 3:
            wait_landed(wrecv.at[0:half], sem_w, 1)
        pair_copy(j).wait_recv()
        pair_copy(pairs + j).wait_recv()
        source = 2 * layers[j] + core
        gate_pre = pair_t[j, :, :f].astype(jnp.float32) + pair_in_t[j, :, :f].astype(jnp.float32)
        up_pre = pair_t[j, :, f:].astype(jnp.float32) + pair_in_t[j, :, f:].astype(jnp.float32)
        grad_scaled = pair_c[j].astype(jnp.float32) + pair_in_c[j].astype(jnp.float32)
        weights = jnp.broadcast_to(wrecv[source][0:1], (LANES, LANES)).T
        w = weights[:cap]
        for r in range(1, per_row):
            w = jnp.where(lax.rem(ep, per_row) == r, weights[r * cap:(r + 1) * cap], w)
        w = w[:, 0:1]
        sigmoid = jax.nn.sigmoid(gate_pre)
        silu = gate_pre * sigmoid
        hidden = silu * up_pre
        grad_hidden = w * grad_scaled
        rows = block(source)
        acts[rows, :f] = (w * hidden).astype(jnp.bfloat16)
        acts[rows, f:2 * f] = (
            grad_hidden * up_pre * sigmoid * (1.0 + gate_pre * (1.0 - sigmoid))
        ).astype(jnp.bfloat16)
        acts[rows, 2 * f:] = (grad_hidden * silu).astype(jnp.bfloat16)
        act_copy(j).start()
        total = jnp.sum(hidden * grad_scaled, axis=1, keepdims=True)
        wide = jnp.concatenate([jnp.broadcast_to(total, (cap, LANES))] * per_row, axis=0)
        comb[source] = wide.T[:8]
        comb_send(source, mate)
        if j:
            comb_send(source, tp)
        else:
            @pl.when(source == ep)
            def _():
                comb_ret[ep] = comb[ep]

            @pl.when(source != ep)
            def _():
                comb_send(source, tp)

    def slot_rows(j, half_of):
        source = 2 * layers[j] + half_of
        rows = block(source)
        slot[rows] = dot(acts[rows, f:], w_slot[...], 1, 0).astype(jnp.bfloat16)

        def send():
            remote(slot.at[rows], ret.at[block(ep)], sem_ret, 1, 0, (source, tp)).start()

        if j:
            send()
        else:
            pl.when(source != ep)(send)

            @pl.when(source == ep)
            def _():
                ret[block(ep)] = slot[rows]

    def slots_own(j, gate):
        slot_rows(j, core)

    def slots_mate(j, gate):
        act_copy(j).wait_recv()
        slot_rows(j, 1 - core)

    def tables(k, gate):
        relay_table(k)

    def grads(which, gate):
        if which == 0:
            down_grad[...] = dot(acts[:, :f], recv_c[...], 0, 0)
        elif which == 1:
            gate_grad[...] = dot(recv_t[...], acts[:, f:2 * f], 0, 0)
        else:
            up_grad[...] = dot(recv_t[...], acts[:, 2 * f:], 0, 0)

    def near_sends(k, gate):
        for d in range(half - 1, 1, -1):
            near_send(k, d)

    names = {
        "n": near_sends,
        "w": weights_out,
        "T": tables, "rt": relay_tokens, "rc": relay_cots, "pt": parts_tokens, "pc": parts_cots,
        "st": pair_tokens, "sc": pair_cots, "a": act, "o": slots_own, "b": slots_mate,
        "g": grads,
    }
    outer_order = (
        "n0", "n1", "pt0", "st0", "pt1", "w0", "pc0", "sc0", "st1", "pc1", "sc1", "a0",
        "o0", "pt3", "w1", "st3", "b0", "pc3", "a1", "o1", "sc3", "b1", "pt2", "a3",
        "o3", "st2", "pc2", "sc2", "b3", "a2", "o2", "b2",
    )
    inner_low = (
        "n0", "n1", "pt0", "w0", "T1", "T0", "st0", "pc0", "rt1", "sc0", "rc1", "a0",
        "o0", "rt0", "pt3", "w1", "rc0", "st3", "b0", "pc3", "sc3", "pt1", "st1", "pt2",
        "st2", "pc1", "a3", "o3", "sc1", "pc2", "b3", "sc2", "a1", "o1", "a2", "o2",
        "b1", "b2",
    )
    inner_high = (
        "n0", "n1", "pt0", "w0", "T1", "T0", "st0", "pc0", "rt1", "sc0", "rc1", "a0",
        "o0", "pt3", "w1", "st3", "rt0", "b0", "rc0", "pc3", "sc3", "pt1", "st1", "pt2",
        "st2", "pc1", "a3", "o3", "b3", "pc2", "sc1", "sc2", "a1", "o1", "a2", "o2",
        "b1", "b2",
    )
    for low, order, gate in (
        (True, outer_order, False), (False, outer_order, False), (True, inner_low, True),
        (False, inner_high, True),
    ):
        role = jnp.logical_and(is_inner if gate else is_outer, side_of == (0 if low else 1))

        @pl.when(role)
        def _():
            for word in order:
                with jax.named_scope(word):
                    names[word[:-1]](int(word[-1]), gate)

    for which in range(3):
        with jax.named_scope("g%d" % which):
            grads(which, None)

    with jax.named_scope("cret"):
        own_half = core == column

        @pl.when(own_half)
        def _():
            wait_landed(comb_ret.at[0:peers - 1], sem_cret, 0)

        @pl.when(jnp.logical_not(own_half))
        def _():
            wait_landed(comb_ret, sem_cret, 0)

    part_lane = lax.broadcasted_iota(jnp.int32, (1, LANES), 1)
    totals = [jnp.zeros((1, tokens.shape[0]), jnp.float32)] * 2
    for q in range(slots // LANES):
        row = comb_ret[q * per_row][0:1]
        for r in range(1, per_row):
            row = jnp.where(part_lane >= r * cap, comb_ret[q * per_row + r][0:1], row)
        values = jnp.broadcast_to(row, (LANES, LANES)).T[:, 0:1]
        for k in range(2):
            chosen = onehot_k[k, q * LANES:(q + 1) * LANES] * values
            totals[k] = totals[k] + jnp.sum(chosen, axis=0, keepdims=True)
    for k in range(2):
        grad_combine[k:k + 1] = totals[k]
    with jax.named_scope("ret"):
        wait_landed(ret.at[block(0, (peers - 1) * cap)], sem_ret, 0)
    with jax.named_scope("sends"):
        send_e.wait_send()
        wait_sent(send_t.at[block(0, (half - 1) * cap)], sem_t, 2)
        wait_sent(send_c.at[block(0, (half - 1) * cap)], sem_c, 2)
        wait_sent(cross_t, sem_x, 4)
        wait_sent(wrecv.at[0:peers - 1], sem_w, 2)
        wait_sent(core_t, sem_core, 2 * pairs)
        wait_sent(core_c, sem_core, 2 * pairs + 1)
        wait_sent(pair_t, sem_pair, 2 * pairs)
        wait_sent(pair_c, sem_pair, 2 * pairs + 1)
        wait_sent(acts.at[block(0, pairs * cap)], sem_act, pairs)
        wait_sent(slot.at[block(0, (peers - 1) * cap)], sem_ret, 1)

        @pl.when(own_half)
        def _():
            wait_sent(comb.at[0:peers - 1], sem_cret, 1)

        @pl.when(jnp.logical_not(own_half))
        def _():
            wait_sent(comb, sem_cret, 1)

        @pl.when(is_inner)
        def _():
            wait_sent(recv_t.at[block(0, 2 * (half - 1) * cap)], sem_rt, 2)
            wait_sent(recv_t.at[block(0, 2 * (half - 1) * cap)], sem_rc, 2)


def store_kernel(ret, gather, *refs):
    count = (len(refs) - 2) // 2
    sources, first, targets = refs[:count], refs[count], refs[count + 1:2 * count + 1]
    grad_tokens, sems = refs[-2:]
    copies = [
        pltpu.make_async_copy(source, target, sems.at[i])
        for i, (source, target) in enumerate(zip((*sources, grad_tokens), (*targets, first)))
    ]
    for copy in copies[:count]:
        copy.start()
    grad_tokens[...] = dot(gather[...], ret[...], 0, 0).astype(jnp.bfloat16)
    copies[count].start()
    for copy in copies:
        copy.wait()


def fused_body(peers, parts, tokens, cotangent, experts, combine, w_gate, w_up, w_down):
    count, width = tokens.shape
    f = w_gate.shape[2]
    picks = experts.shape[1]
    cap = 2 * count * picks // peers
    slots = peers * cap
    pairs = peers // 2
    bf16, f32 = jnp.bfloat16, jnp.float32
    dma = pltpu.SemaphoreType.DMA
    vmem = pl.BlockSpec(memory_space=pltpu.VMEM)
    hbm = pl.BlockSpec(memory_space=pltpu.HBM)
    shapes = (
        jax.ShapeDtypeStruct((count, width), bf16),
        jax.ShapeDtypeStruct((picks, count), f32),
        jax.ShapeDtypeStruct((width, f), f32),
        jax.ShapeDtypeStruct((width, f), f32),
        jax.ShapeDtypeStruct((f, width), f32),
    )
    half_rows = pltpu.VMEM((slots // 2, width), bf16)
    relayed = pltpu.VMEM((2, slots // 2, width), bf16)
    rows = pltpu.VMEM((count, width), bf16)
    crossed = pltpu.VMEM((2, count, width), bf16)
    landed = pltpu.VMEM((slots, width), bf16)
    sums_t = pltpu.VMEM((pairs, cap, 2 * f), bf16)
    sums_c = pltpu.VMEM((pairs, cap, f), bf16)
    small = pltpu.VMEM((peers, 8, LANES), f32)
    outs = pl.pallas_call(
        functools.partial(fused_kernel, peers, parts),
        out_shape=(
            jax.ShapeDtypeStruct((slots, width), bf16), jax.ShapeDtypeStruct((slots, count), bf16),
            *shapes[1:],
        ),
        in_specs=[hbm] * 7,
        out_specs=(vmem,) * 6,
        scratch_shapes=[
            rows, rows, pltpu.VMEM((picks, count), jnp.int32), pltpu.VMEM((picks, count), f32),
            pltpu.VMEM((width, f), bf16), pltpu.VMEM((width, f), bf16), pltpu.VMEM((f, width), bf16),
            pltpu.VMEM((2 * f, width), bf16), pltpu.VMEM((width, f), bf16),
            half_rows, half_rows, crossed, crossed, pltpu.VMEM((2, picks, count), jnp.int32),
            relayed, relayed, landed, landed,
            pltpu.VMEM((slots // LANES, 8, LANES), f32), small,
            pltpu.VMEM((pairs, 2 * cap, 2 * f), bf16), pltpu.VMEM((pairs, 2 * cap, f), bf16),
            sums_t, sums_c, sums_t, sums_c, sums_t, sums_c,
            pltpu.VMEM((slots, 3 * f), bf16), small, landed,
            small, pltpu.VMEM((2, slots // 2, count), bf16),
            pltpu.VMEM((picks, slots, count), f32),
            dma((7,)), dma((3,)), dma((3,)), dma((3,)), dma((3,)), dma((5,)), dma((3,)), dma((3,)),
            dma((2 * pairs + 2,)), dma((2 * pairs + 2,)), dma((pairs + 1,)), dma((2,)), dma((2,)),
        ],
        compiler_params=pltpu.CompilerParams(
            collective_id=0, has_side_effects=True, vmem_limit_bytes=48 * 1024 * 1024
        ),
    )(*(
        pltpu.with_memory_space_constraint(x, pltpu.HBM)
        for x in (tokens, cotangent, experts.T, combine.T, w_gate, w_up, w_down)
    ))
    outs = pl.pallas_call(
        store_kernel,
        out_shape=shapes,
        in_specs=[vmem] * 6,
        out_specs=(hbm,) * 5,
        scratch_shapes=[rows, dma((5,))],
        compiler_params=pltpu.CompilerParams(vmem_limit_bytes=4 * 1024 * 1024),
    )(*outs)
    return outs[0], outs[1].T, outs[2][None], outs[3][None], outs[4][None]


def choose(mesh, tokens, cotangent, experts, combine, w_gate, w_up, w_down):
    peers, parts = mesh.shape["ep"], mesh.shape["tp"]
    count, width = tokens.shape
    cap = 2 * count * experts.shape[1] // w_gate.shape[0] // peers
    fits = (
        w_gate.shape[0] == 1 and experts.shape[1] == 2 and parts == 4
        and peers == 8 and cap in (16, 32, 64, 128)
        and count % LANES == 0 and width % LANES == 0
        and w_gate.shape[2] % LANES == 0 and peers * cap % LANES == 0
    )
    run = functools.partial(fused_body, peers, parts) if fits else body
    return run(tokens, cotangent, experts, combine, w_gate, w_up, w_down)


def solution(mesh):
    return jax.shard_map(
        functools.partial(choose, mesh),
        mesh=mesh,
        in_specs=(
            P("ep", "tp"),
            P("ep", "tp"),
            P("ep", None),
            P("ep", None),
            P("ep", "tp", None),
            P("ep", "tp", None),
            P("ep", None, "tp"),
        ),
        out_specs=(
            P("ep", "tp"),
            P("ep", None),
            P("ep", "tp", None),
            P("ep", "tp", None),
            P("ep", None, "tp"),
        ),
        check_vma=False,
    )
```

```python
import functools

import jax
import jax.numpy as jnp
from jax import lax
from jax.experimental import pallas as pl
from jax.experimental.pallas import tpu as pltpu
from jax.sharding import PartitionSpec as P


def slot_positions(routed, total_experts, capacity):
    onehot = (routed[:, None] == jnp.arange(total_experts, dtype=jnp.int32)[None, :]).astype(
        jnp.int32
    )
    earlier = jnp.sum((jnp.cumsum(onehot, axis=0) - onehot) * onehot, axis=1)
    return routed * capacity + earlier


def activation(gate_pre, up_pre, grad_scaled, weight_grid):
    sigmoid_val = jax.nn.sigmoid(gate_pre)
    silu_val = gate_pre * sigmoid_val
    hidden = silu_val * up_pre
    scaled = (weight_grid * hidden).astype(jnp.bfloat16)
    comb_part = jnp.sum(hidden * grad_scaled, axis=3)
    grad_hidden = weight_grid * grad_scaled
    grad_gate_pre = (
        grad_hidden * up_pre * sigmoid_val * (1.0 + gate_pre * (1.0 - sigmoid_val))
    ).astype(jnp.bfloat16)
    grad_up_pre = (grad_hidden * silu_val).astype(jnp.bfloat16)
    return (scaled, grad_gate_pre, grad_up_pre, comb_part)


def body(tokens, cotangent, experts, combine, w_gate, w_up, w_down):
    peers = lax.axis_size("ep")
    local_experts = w_gate.shape[0]
    total_experts = local_experts * peers
    tok_count = tokens.shape[0]
    picks = experts.shape[1]
    assigns = tok_count * picks
    capacity = 2 * assigns // total_experts
    per_peer = local_experts * capacity
    block_width = tokens.shape[1]
    slot_index = slot_positions(experts.reshape(assigns), total_experts, capacity)
    slot_owner = (
        jnp.zeros((total_experts * capacity,), jnp.int32)
        .at[slot_index]
        .set(jnp.arange(assigns, dtype=jnp.int32) + 1)
    )
    filled = slot_owner > 0
    source = jnp.maximum(slot_owner - 1, 0)
    token_ids = source // picks
    filled_col = filled[:, None]
    send_rows = jnp.where(
        filled_col, jnp.take(tokens, token_ids, axis=0), jnp.zeros((), jnp.bfloat16)
    ).reshape(peers, per_peer, block_width)
    send_cots = jnp.where(
        filled_col, jnp.take(cotangent, token_ids, axis=0), jnp.zeros((), jnp.bfloat16)
    ).reshape(peers, per_peer, block_width)
    send_weights = (
        jnp.where(filled, jnp.take(combine.reshape(assigns), source), jnp.float32(0.0))
        .astype(jnp.bfloat16)
        .reshape(peers, per_peer)
    )
    recv_rows, recv_cots, recv_weights = (
        lax.all_to_all(send_rows, "ep", split_axis=0, concat_axis=0, tiled=True),
        lax.all_to_all(send_cots, "ep", split_axis=0, concat_axis=0, tiled=True),
        lax.all_to_all(send_weights, "ep", split_axis=0, concat_axis=0, tiled=True),
    )
    rows_grid = recv_rows.reshape(peers, local_experts, capacity, block_width)
    cots_grid = recv_cots.reshape(peers, local_experts, capacity, block_width)
    weight_grid = recv_weights.astype(jnp.float32).reshape(peers, local_experts, capacity, 1)
    gate_part = jnp.einsum(
        "secd,edf->secf", rows_grid, w_gate, preferred_element_type=jnp.float32
    ).astype(jnp.bfloat16)
    up_part = jnp.einsum(
        "secd,edf->secf", rows_grid, w_up, preferred_element_type=jnp.float32
    ).astype(jnp.bfloat16)
    down_part = jnp.einsum(
        "secd,efd->secf", cots_grid, w_down, preferred_element_type=jnp.float32
    ).astype(jnp.bfloat16)
    gate_pre, up_pre, grad_scaled = (
        lax.psum(gate_part, "tp").astype(jnp.float32),
        lax.psum(up_part, "tp").astype(jnp.float32),
        lax.psum(down_part, "tp").astype(jnp.float32),
    )
    scaled, grad_gate_pre, grad_up_pre, comb_part = activation(
        gate_pre, up_pre, grad_scaled, weight_grid
    )
    down_grad = jnp.einsum("secf,secd->efd", scaled, cots_grid, preferred_element_type=jnp.float32)
    gate_grad = jnp.einsum(
        "secd,secf->edf", rows_grid, grad_gate_pre, preferred_element_type=jnp.float32
    )
    up_grad = jnp.einsum(
        "secd,secf->edf", rows_grid, grad_up_pre, preferred_element_type=jnp.float32
    )
    slot_sum = jnp.einsum(
        "secf,edf->secd", grad_gate_pre, w_gate, preferred_element_type=jnp.float32
    )
    slot_sum = slot_sum + jnp.einsum(
        "secf,edf->secd", grad_up_pre, w_up, preferred_element_type=jnp.float32
    )
    slot_grad = slot_sum.astype(jnp.bfloat16).reshape(peers, per_peer, block_width)
    returned = lax.all_to_all(slot_grad, "ep", split_axis=0, concat_axis=0, tiled=True)
    comb_back = lax.all_to_all(
        comb_part.reshape(peers, per_peer), "ep", split_axis=0, concat_axis=0, tiled=True
    )
    full_grad = returned.reshape(total_experts * capacity, block_width)
    per_assign = (
        jnp.take(full_grad, slot_index, axis=0)
        .astype(jnp.float32)
        .reshape(tok_count, picks, block_width)
    )
    grad_tokens = jnp.sum(per_assign, axis=1).astype(jnp.bfloat16)
    grad_combine = jnp.take(comb_back.reshape(total_experts * capacity), slot_index).reshape(
        tok_count, picks
    )
    return (grad_tokens, grad_combine, gate_grad, up_grad, down_grad)


MESH = pl.DeviceIdType.MESH
LANES = 128


def flip(index, mask, count):
    result, bit = 0, 1
    while bit < count:
        digit = lax.rem(lax.div(index, bit), 2)
        result = result + bit * ((1 - digit) if mask & bit else digit)
        bit *= 2
    return result


def dot(a, b, ca, cb):
    return lax.dot_general(a, b, (((ca,), (cb,)), ((), ())), preferred_element_type=jnp.float32)


def slot_table(first_expert, second_expert, base, slots, cap):
    count = first_expert.shape[1]
    row = lax.broadcasted_iota(jnp.int32, (slots, count), 0)
    expert = base + lax.shift_right_logical(row, cap.bit_length() - 1)
    number = jnp.bitwise_and(row, cap - 1).astype(jnp.float32)
    first = jnp.where(first_expert == expert, 1.0, 0.0)
    second = jnp.where(second_expert == expert, 1.0, 0.0)
    earlier = jnp.where(
        lax.broadcasted_iota(jnp.int32, (count, count), 0)
        < lax.broadcasted_iota(jnp.int32, (count, count), 1), 1.0, 0.0
    ).astype(jnp.bfloat16)
    position = dot((first + second).astype(jnp.bfloat16), earlier, 1, 0)
    here = jnp.where(position == number, 1.0, 0.0)
    return first * here, second * here


def fused_kernel(
    peers, parts, tokens_hbm, cotangent_hbm, experts_hbm, combine_hbm, gate_hbm, up_hbm, down_hbm,
    ret, gather, grad_combine, gate_grad, up_grad, down_grad,
    tokens, cotangent, experts, combine, w_gate, w_up, w_down, w_slot, w_part,
    send_t, send_c, cross_t, cross_c, cross_e, relay_t, relay_c, recv_t, recv_c,
    wsend, wrecv, part_t, part_c, core_t, core_c, pair_t, pair_c, pair_in_t, pair_in_c,
    acts, comb, slot,
    comb_ret, gather_relay, onehot_k,
    sem_in, sem_t, sem_c, sem_rt, sem_rc, sem_x, sem_w, sem_e,
    sem_core, sem_pair, sem_act, sem_ret, sem_cret,
):
    ep, tp = lax.axis_index("ep"), lax.axis_index("tp")
    core = lax.rem(tp, 2)
    mate = tp + 1 - 2 * core
    across = lax.rem(tp + 2, parts)
    f = w_gate.shape[1]
    slots = recv_t.shape[0]
    cap = slots // peers
    half = peers // 2
    per_row = LANES // cap
    side_of, place = lax.div(ep, half), lax.rem(ep, half)
    peer = [flip(ep, d, peers) for d in range(peers)]
    spot = [lax.rem(p, half) for p in peer]
    layer, column = lax.div(ep, 2), lax.rem(ep, 2)
    inner = jnp.where(layer == 1 + side_of, 1, 0)
    is_inner, is_outer = inner == 1, inner == 0
    layers = (layer, layer + 1 - 2 * lax.rem(layer, 2), 2 - side_of, 3 * (1 - side_of))
    far_gate = (2 * layers[2] + column, tp)

    def block(index, size=cap):
        return pl.ds(pl.multiple_of(index * size, size), size)

    def remote(src, dst, sems, sent, landed, device):
        return pltpu.make_async_remote_copy(
            src_ref=src, dst_ref=dst, send_sem=sems.at[sent], recv_sem=sems.at[landed],
            device_id=device, device_id_type=MESH,
        )

    def wait_sent(ref, sems, sent):
        remote(ref, ref, sems, sent, sent, (ep, mate)).wait_send()

    def wait_landed(ref, sems, landed):
        remote(ref, ref, sems, landed, landed, (ep, mate)).wait_recv()

    loads = [
        pltpu.make_async_copy(source, target, sem_in.at[max(i // 2, i - 2)])
        for i, (source, target) in enumerate((
            (experts_hbm, experts), (combine_hbm, combine), (tokens_hbm, tokens),
            (cotangent_hbm, cotangent), (gate_hbm.at[0], w_gate), (up_hbm.at[0], w_up),
            (down_hbm.at[0], w_down),
        ))
    ]
    barrier = pltpu.get_barrier_semaphore()
    for device in [(peer[d], tp) for d in range(1, half)] + [(ep, mate), (ep, across)]:
        pl.semaphore_signal(barrier, inc=1, device_id=device, device_id_type=MESH)

    @pl.when(is_inner)
    def _():
        for far in (2, 3):
            device = (2 * layers[far] + column, tp)
            pl.semaphore_signal(barrier, inc=1, device_id=device, device_id_type=MESH)

    for load in loads:
        load.start()
    wait_landed(cross_e, sem_in, 0)

    first, second = slot_table(experts[0:1], experts[1:2], 0, slots, cap)
    onehot_k[0] = first
    onehot_k[1] = second
    gather[...] = (first + second).astype(jnp.bfloat16)
    weight = combine[...].astype(jnp.bfloat16).astype(jnp.float32)
    weight_column = jnp.sum(first * weight[0:1] + second * weight[1:2], axis=1, keepdims=True)
    for q in range(slots // LANES):
        wide = jnp.broadcast_to(weight_column[q * LANES:(q + 1) * LANES], (LANES, LANES))
        wsend[q] = wide.T[:8]
    wrecv[ep] = wsend[lax.div(ep, per_row)]
    wait_landed(cross_t, sem_in, 1)
    own = gather[block(side_of, half * cap)]
    send_t[...] = dot(own, tokens[...], 1, 0).astype(jnp.bfloat16)
    send_c[...] = dot(own, cotangent[...], 1, 0).astype(jnp.bfloat16)
    with jax.named_scope("barrier"):
        pl.semaphore_wait(barrier, half + 2)

    send_e = remote(experts, cross_e.at[1 - inner], sem_e, 2, 1 - inner, far_gate)
    send_e.start()

    def send_weights(target, far):
        remote(
            wsend.at[lax.div(target, per_row)], wrecv.at[ep], sem_w, 2, far, (target, tp)
        ).start()

    for d in range(1, half):
        send_weights(peer[d], 0)
    remote(tokens, cross_t.at[1 - inner], sem_x, 4, 1 - inner, far_gate).start()
    remote(cotangent, cross_c.at[1 - inner], sem_x, 4, 3 - inner, far_gate).start()

    def near_send(k, d):
        packed, landed, sems = ((send_t, recv_t, sem_t), (send_c, recv_c, sem_c))[k]
        remote(
            packed.at[block(spot[d])], landed.at[block(ep)], sems, 2, min(d - 1, 1), (peer[d], tp)
        ).start()

    near_send(0, 1)
    near_send(1, 1)
    recv_t[block(ep)] = send_t[block(place)]
    recv_c[block(ep)] = send_c[block(place)]

    for load in loads[4:]:
        load.wait()
    with jax.named_scope("transposes"):
        w_slot[:f] = w_gate[...].T
        w_slot[f:] = w_up[...].T
        w_part[...] = w_down[...].T

    def relay_table(k):
        wait_landed(cross_e.at[k], sem_e, k)
        chosen_a, chosen_b = slot_table(
            cross_e[k, 0:1], cross_e[k, 1:2], side_of * half, half * cap, cap
        )
        gather_relay[k] = (chosen_a + chosen_b).astype(jnp.bfloat16)

    def relay(k, landed_in, crossed, packed, landed, sems):
        wait_landed(crossed.at[k], sem_x, landed_in)
        packed[k] = dot(gather_relay[k], crossed[k], 1, 0).astype(jnp.bfloat16)
        rows = block(2 * layers[2 + k] + column)
        for d in (1, 2, 3) if k else (1, 3, 2):
            remote(packed.at[k, block(spot[d])], landed.at[rows], sems, 2, k, (peer[d], tp)).start()
        landed[rows] = packed[k, block(place)]

    def relay_tokens(k, gate):
        relay(k, k, cross_t, relay_t, recv_t, sem_rt)

    def relay_cots(k, gate):
        relay(k, 2 + k, cross_c, relay_c, recv_c, sem_rc)

    def arrive(j, gate, landed, near_sems, sems):
        count = cap if j == 0 or (gate and j > 1) else 2 * cap
        wait_landed(landed.at[block(0, count)], sems if j > 1 else near_sems, j % 2)

    def weights_out(k, gate):
        for b in range(2):
            target = 2 * layers[2 + k] + b
            send_weights(target, 1)

    pairs = peers // 2

    def core_copy(i):
        part, landed = (part_t, core_t) if i < pairs else (part_c, core_c)
        j = i % pairs
        return remote(
            part.at[j, block(1 - core)], landed.at[j], sem_core, 2 * pairs, i, (ep, mate)
        )

    def pair_copy(i):
        summed, landed = (pair_t, pair_in_t) if i < pairs else (pair_c, pair_in_c)
        return remote(
            summed.at[i % pairs], landed.at[i % pairs], sem_pair, 2 * pairs, i,
            (ep, across),
        )

    def act_copy(j):
        rows = block(2 * layers[j] + core)
        return remote(acts.at[rows], acts.at[rows], sem_act, pairs, j, (ep, mate))

    def comb_send(source, device):
        remote(comb.at[source], comb_ret.at[ep], sem_cret, 1, 0, (source, device)).start()

    def parts_tokens(j, gate):
        arrive(j, gate, recv_t, sem_t, sem_rt)
        rows = recv_t[block(layers[j], 2 * cap)]
        part_t[j, :, :f] = dot(rows, w_gate[...], 1, 0).astype(jnp.bfloat16)
        part_t[j, :, f:] = dot(rows, w_up[...], 1, 0).astype(jnp.bfloat16)
        core_copy(j).start()

    def parts_cots(j, gate):
        arrive(j, gate, recv_c, sem_c, sem_rc)
        cots = recv_c[block(layers[j], 2 * cap)]
        part_c[j] = dot(cots, w_part[...], 1, 0).astype(jnp.bfloat16)
        core_copy(pairs + j).start()

    def pair_sum(j, i, part, landed, summed):
        core_copy(i).wait_recv()
        mine = part[j, block(core)].astype(jnp.float32)
        summed[j] = (mine + landed[j].astype(jnp.float32)).astype(jnp.bfloat16)
        pair_copy(i).start()

    def pair_tokens(j, gate):
        pair_sum(j, j, part_t, core_t, pair_t)

    def pair_cots(j, gate):
        pair_sum(j, pairs + j, part_c, core_c, pair_c)

    def act(j, gate):
        if j == 0:
            wait_landed(wrecv.at[0:half - 1], sem_w, 0)
        if j == 3:
            wait_landed(wrecv.at[0:half], sem_w, 1)
        pair_copy(j).wait_recv()
        pair_copy(pairs + j).wait_recv()
        source = 2 * layers[j] + core
        gate_pre = pair_t[j, :, :f].astype(jnp.float32) + pair_in_t[j, :, :f].astype(jnp.float32)
        up_pre = pair_t[j, :, f:].astype(jnp.float32) + pair_in_t[j, :, f:].astype(jnp.float32)
        grad_scaled = pair_c[j].astype(jnp.float32) + pair_in_c[j].astype(jnp.float32)
        weights = jnp.broadcast_to(wrecv[source][0:1], (LANES, LANES)).T
        w = weights[:cap]
        for r in range(1, per_row):
            w = jnp.where(lax.rem(ep, per_row) == r, weights[r * cap:(r + 1) * cap], w)
        w = w[:, 0:1]
        sigmoid = jax.nn.sigmoid(gate_pre)
        silu = gate_pre * sigmoid
        hidden = silu * up_pre
        grad_hidden = w * grad_scaled
        rows = block(source)
        acts[rows, :f] = (w * hidden).astype(jnp.bfloat16)
        acts[rows, f:2 * f] = (
            grad_hidden * up_pre * sigmoid * (1.0 + gate_pre * (1.0 - sigmoid))
        ).astype(jnp.bfloat16)
        acts[rows, 2 * f:] = (grad_hidden * silu).astype(jnp.bfloat16)
        act_copy(j).start()
        total = jnp.sum(hidden * grad_scaled, axis=1, keepdims=True)
        wide = jnp.concatenate([jnp.broadcast_to(total, (cap, LANES))] * per_row, axis=0)
        comb[source] = wide.T[:8]
        comb_send(source, mate)
        if j:
            comb_send(source, tp)
        else:
            @pl.when(source == ep)
            def _():
                comb_ret[ep] = comb[ep]

            @pl.when(source != ep)
            def _():
                comb_send(source, tp)

    def slot_rows(j, half_of):
        source = 2 * layers[j] + half_of
        rows = block(source)
        slot[rows] = dot(acts[rows, f:], w_slot[...], 1, 0).astype(jnp.bfloat16)

        def send():
            remote(slot.at[rows], ret.at[block(ep)], sem_ret, 1, 0, (source, tp)).start()

        if j:
            send()
        else:
            pl.when(source != ep)(send)

            @pl.when(source == ep)
            def _():
                ret[block(ep)] = slot[rows]

    def slots_own(j, gate):
        slot_rows(j, core)

    def slots_mate(j, gate):
        act_copy(j).wait_recv()
        slot_rows(j, 1 - core)

    def tables(k, gate):
        relay_table(k)

    def grads(which, gate):
        if which == 0:
            down_grad[...] = dot(acts[:, :f], recv_c[...], 0, 0)
        elif which == 1:
            gate_grad[...] = dot(recv_t[...], acts[:, f:2 * f], 0, 0)
        else:
            up_grad[...] = dot(recv_t[...], acts[:, 2 * f:], 0, 0)

    def near_sends(k, gate):
        for d in range(half - 1, 1, -1):
            near_send(k, d)

    names = {
        "n": near_sends,
        "w": weights_out,
        "T": tables, "rt": relay_tokens, "rc": relay_cots, "pt": parts_tokens, "pc": parts_cots,
        "st": pair_tokens, "sc": pair_cots, "a": act, "o": slots_own, "b": slots_mate,
        "g": grads,
    }
    outer_order = (
        "n0", "n1", "pt0", "st0", "pt1", "w0", "pc0", "sc0", "st1", "pc1", "sc1", "a0",
        "o0", "pt3", "w1", "st3", "b0", "pc3", "a1", "o1", "sc3", "b1", "pt2", "a3",
        "o3", "st2", "pc2", "sc2", "b3", "a2", "o2", "b2",
    )
    inner_low = (
        "n0", "n1", "pt0", "w0", "T1", "T0", "st0", "pc0", "rt1", "sc0", "rc1", "a0",
        "o0", "rt0", "pt3", "w1", "rc0", "st3", "b0", "pc3", "sc3", "pt1", "st1", "pt2",
        "st2", "pc1", "a3", "o3", "sc1", "pc2", "b3", "sc2", "a1", "o1", "a2", "o2",
        "b1", "b2",
    )
    inner_high = (
        "n0", "n1", "pt0", "w0", "T1", "T0", "st0", "pc0", "rt1", "sc0", "rc1", "a0",
        "o0", "pt3", "w1", "st3", "rt0", "b0", "rc0", "pc3", "sc3", "pt1", "st1", "pt2",
        "st2", "pc1", "a3", "o3", "b3", "pc2", "sc1", "sc2", "a1", "o1", "a2", "o2",
        "b1", "b2",
    )
    for low, order, gate in (
        (True, outer_order, False), (False, outer_order, False), (True, inner_low, True),
        (False, inner_high, True),
    ):
        role = jnp.logical_and(is_inner if gate else is_outer, side_of == (0 if low else 1))

        @pl.when(role)
        def _():
            for word in order:
                with jax.named_scope(word):
                    names[word[:-1]](int(word[-1]), gate)

    for which in range(3):
        with jax.named_scope("g%d" % which):
            grads(which, None)

    with jax.named_scope("cret"):
        own_half = core == column

        @pl.when(own_half)
        def _():
            wait_landed(comb_ret.at[0:peers - 1], sem_cret, 0)

        @pl.when(jnp.logical_not(own_half))
        def _():
            wait_landed(comb_ret, sem_cret, 0)

    part_lane = lax.broadcasted_iota(jnp.int32, (1, LANES), 1)
    totals = [jnp.zeros((1, tokens.shape[0]), jnp.float32)] * 2
    for q in range(slots // LANES):
        row = comb_ret[q * per_row][0:1]
        for r in range(1, per_row):
            row = jnp.where(part_lane >= r * cap, comb_ret[q * per_row + r][0:1], row)
        values = jnp.broadcast_to(row, (LANES, LANES)).T[:, 0:1]
        for k in range(2):
            chosen = onehot_k[k, q * LANES:(q + 1) * LANES] * values
            totals[k] = totals[k] + jnp.sum(chosen, axis=0, keepdims=True)
    for k in range(2):
        grad_combine[k:k + 1] = totals[k]
    with jax.named_scope("ret"):
        wait_landed(ret.at[block(0, (peers - 1) * cap)], sem_ret, 0)
    with jax.named_scope("sends"):
        send_e.wait_send()
        wait_sent(send_t.at[block(0, (half - 1) * cap)], sem_t, 2)
        wait_sent(send_c.at[block(0, (half - 1) * cap)], sem_c, 2)
        wait_sent(cross_t, sem_x, 4)
        wait_sent(wrecv.at[0:peers - 1], sem_w, 2)
        wait_sent(acts.at[block(0, pairs * cap)], sem_core, 2 * pairs)
        wait_sent(acts.at[block(0, pairs * cap)], sem_pair, 2 * pairs)
        wait_sent(acts.at[block(0, pairs * cap)], sem_act, pairs)
        wait_sent(slot.at[block(0, (peers - 1) * cap)], sem_ret, 1)

        @pl.when(own_half)
        def _():
            wait_sent(comb.at[0:peers - 1], sem_cret, 1)

        @pl.when(jnp.logical_not(own_half))
        def _():
            wait_sent(comb, sem_cret, 1)

        @pl.when(is_inner)
        def _():
            wait_sent(recv_t.at[block(0, 2 * (half - 1) * cap)], sem_rt, 2)
            wait_sent(recv_t.at[block(0, 2 * (half - 1) * cap)], sem_rc, 2)


def store_kernel(ret, gather, *refs):
    count = (len(refs) - 2) // 2
    sources, first, targets = refs[:count], refs[count], refs[count + 1:2 * count + 1]
    grad_tokens, sems = refs[-2:]
    copies = [
        pltpu.make_async_copy(source, target, sems.at[i])
        for i, (source, target) in enumerate(zip((*sources, grad_tokens), (*targets, first)))
    ]
    for copy in copies[:count]:
        copy.start()
    grad_tokens[...] = dot(gather[...], ret[...], 0, 0).astype(jnp.bfloat16)
    copies[count].start()
    for copy in copies:
        copy.wait()


def fused_body(peers, parts, tokens, cotangent, experts, combine, w_gate, w_up, w_down):
    count, width = tokens.shape
    f = w_gate.shape[2]
    picks = experts.shape[1]
    cap = 2 * count * picks // peers
    slots = peers * cap
    pairs = peers // 2
    bf16, f32 = jnp.bfloat16, jnp.float32
    dma = pltpu.SemaphoreType.DMA
    vmem = pl.BlockSpec(memory_space=pltpu.VMEM)
    hbm = pl.BlockSpec(memory_space=pltpu.HBM)
    shapes = (
        jax.ShapeDtypeStruct((count, width), bf16),
        jax.ShapeDtypeStruct((picks, count), f32),
        jax.ShapeDtypeStruct((width, f), f32),
        jax.ShapeDtypeStruct((width, f), f32),
        jax.ShapeDtypeStruct((f, width), f32),
    )
    half_rows = pltpu.VMEM((slots // 2, width), bf16)
    relayed = pltpu.VMEM((2, slots // 2, width), bf16)
    rows = pltpu.VMEM((count, width), bf16)
    crossed = pltpu.VMEM((2, count, width), bf16)
    landed = pltpu.VMEM((slots, width), bf16)
    sums_t = pltpu.VMEM((pairs, cap, 2 * f), bf16)
    sums_c = pltpu.VMEM((pairs, cap, f), bf16)
    small = pltpu.VMEM((peers, 8, LANES), f32)
    outs = pl.pallas_call(
        functools.partial(fused_kernel, peers, parts),
        out_shape=(
            jax.ShapeDtypeStruct((slots, width), bf16), jax.ShapeDtypeStruct((slots, count), bf16),
            *shapes[1:],
        ),
        in_specs=[hbm] * 7,
        out_specs=(vmem,) * 6,
        scratch_shapes=[
            rows, rows, pltpu.VMEM((picks, count), jnp.int32), pltpu.VMEM((picks, count), f32),
            pltpu.VMEM((width, f), bf16), pltpu.VMEM((width, f), bf16), pltpu.VMEM((f, width), bf16),
            pltpu.VMEM((2 * f, width), bf16), pltpu.VMEM((width, f), bf16),
            half_rows, half_rows, crossed, crossed, pltpu.VMEM((2, picks, count), jnp.int32),
            relayed, relayed, landed, landed,
            pltpu.VMEM((slots // LANES, 8, LANES), f32), small,
            pltpu.VMEM((pairs, 2 * cap, 2 * f), bf16), pltpu.VMEM((pairs, 2 * cap, f), bf16),
            sums_t, sums_c, sums_t, sums_c, sums_t, sums_c,
            pltpu.VMEM((slots, 3 * f), bf16), small, landed,
            small, pltpu.VMEM((2, slots // 2, count), bf16),
            pltpu.VMEM((picks, slots, count), f32),
            dma((5,)), dma((3,)), dma((3,)), dma((3,)), dma((3,)), dma((5,)), dma((3,)), dma((3,)),
            dma((2 * pairs + 1,)), dma((2 * pairs + 1,)), dma((pairs + 1,)), dma((2,)), dma((2,)),
        ],
        compiler_params=pltpu.CompilerParams(
            collective_id=0, has_side_effects=True, vmem_limit_bytes=48 * 1024 * 1024
        ),
    )(*(
        pltpu.with_memory_space_constraint(x, pltpu.HBM)
        for x in (tokens, cotangent, experts.T, combine.T, w_gate, w_up, w_down)
    ))
    outs = pl.pallas_call(
        store_kernel,
        out_shape=shapes,
        in_specs=[vmem] * 6,
        out_specs=(hbm,) * 5,
        scratch_shapes=[rows, dma((5,))],
        compiler_params=pltpu.CompilerParams(vmem_limit_bytes=4 * 1024 * 1024),
    )(*outs)
    return outs[0], outs[1].T, outs[2][None], outs[3][None], outs[4][None]


def choose(mesh, tokens, cotangent, experts, combine, w_gate, w_up, w_down):
    peers, parts = mesh.shape["ep"], mesh.shape["tp"]
    count, width = tokens.shape
    cap = 2 * count * experts.shape[1] // w_gate.shape[0] // peers
    fits = (
        w_gate.shape[0] == 1 and experts.shape[1] == 2 and parts == 4
        and peers == 8 and cap in (16, 32, 64, 128)
        and count % LANES == 0 and width % LANES == 0
        and w_gate.shape[2] % LANES == 0 and peers * cap % LANES == 0
    )
    run = functools.partial(fused_body, peers, parts) if fits else body
    return run(tokens, cotangent, experts, combine, w_gate, w_up, w_down)


def solution(mesh):
    return jax.shard_map(
        functools.partial(choose, mesh),
        mesh=mesh,
        in_specs=(
            P("ep", "tp"),
            P("ep", "tp"),
            P("ep", None),
            P("ep", None),
            P("ep", "tp", None),
            P("ep", "tp", None),
            P("ep", None, "tp"),
        ),
        out_specs=(
            P("ep", "tp"),
            P("ep", None),
            P("ep", "tp", None),
            P("ep", "tp", None),
            P("ep", None, "tp"),
        ),
        check_vma=False,
    )
```
